128 devices in a mesh: sp: 16 (over z, x), tp: 8 (over y, core).
Axes of the slice: x: 4, y: 4, z: 4, core: 2. Of those that a mesh axis runs over, the one named last changes fastest.
Arguments:
- x_in: bfloat16 [16, 6144, 2048], P('tp', 'sp'), may hold values from -13 to 13
- x_new: bfloat16 [16, 2048], P('sp'), may hold values from -6 to 6
- w_x: bfloat16 [2048, 2048], replicated, may hold values from -0.125 to 0.125
- w_b: bfloat16 [2048, 1024], replicated, may hold values from -0.125 to 0.125
- w_c: bfloat16 [2048, 1024], replicated, may hold values from -0.125 to 0.125
- w_dt: bfloat16 [2048, 32], replicated, may hold values from -0.125 to 0.125
- w_z: bfloat16 [2048, 2048], P(None, 'tp'), may hold values from -3 to 3
- conv_w: float32 [4, 4096], replicated, may hold values from -3 to 3
- conv_b: float32 [4096], replicated, may hold values from -3 to 3
- dt_bias: float32 [32], replicated, may hold values from -4 to -2
- a_log: float32 [32], replicated, may hold values from -12 to 0
- d_skip: float32 [32], replicated, may hold values from 1 to 8
- norm_g: float32 [32, 64], P('tp'), may hold values from 0.1 to 1.9
Outputs:
- state_cache: bfloat16 [16, 32, 64, 128], P('sp', 'tp')
- read_out: bfloat16 [16, 32, 64], P('sp', 'tp')
The draws below stay inside these ranges and needn't reach their ends.
All inputs are finite; a program needn't handle non-finite values.
Results may differ from the reference program's by a relative error of at most 0.015.
Values may be sent and summed in bfloat16 or wider, within the bound.
A program may use at most 128 MiB of HBM per device.

```python
import math
import jax
import jax.numpy as jnp
from jax import lax

D = 2048
H = 32
P_SIZE = 64
G = 8
N = 128
KW = 4
POS_DEV = 384
R = 4
SEQS = 16
LENGTH = 6144


def draw_x_in(key, part):
    normal_key, factor_key = jax.random.split(key)
    blocks = LENGTH // POS_DEV
    factor = jnp.exp(jax.random.uniform(factor_key, (SEQS, blocks, 1), jnp.float32, -1.2, 1.2))
    factor = jnp.repeat(factor, POS_DEV, axis=1)
    values = jnp.clip(jax.random.normal(normal_key, (SEQS, LENGTH, D), jnp.float32), -3.9, 3.9) * factor
    return values.astype(jnp.bfloat16)


def draw_a_log(key, part):
    pick_key, fast_key, slow_key = jax.random.split(key, 3)
    pick_draw = jax.random.uniform(pick_key, (H,), jnp.float32)
    fast_share = 0.5
    fast_mag = jnp.exp(jax.random.uniform(fast_key, (H,), jnp.float32, math.log(0.15), math.log(0.5)))
    slow_mag = jnp.exp(jax.random.uniform(slow_key, (H,), jnp.float32, math.log(5.0 / LENGTH), math.log(15.0 / LENGTH)))
    return jnp.log(jnp.where(pick_draw < fast_share, fast_mag, slow_mag)).astype(jnp.float32)


def draw_w_z(key, part):
    entry_key, scale_key = jax.random.split(key)
    col_scale = jnp.exp(jax.random.uniform(scale_key, (1, H * P_SIZE), jnp.float32, -1.2, 1.2))
    entries = jnp.clip(jax.random.normal(entry_key, (D, H * P_SIZE), jnp.float32), -6.0, 6.0)
    return (entries * col_scale * D ** (-0.5)).astype(jnp.bfloat16)


def level_of(key, extent, cuts, least, largest):
    factor_of = 1.0
    for dim, blocks in cuts:
        draws = jax.random.uniform(jax.random.fold_in(jax.random.fold_in(key, 6), dim), (blocks,), jnp.float32, least / len(cuts), largest / len(cuts))
        factor_of = factor_of * jnp.repeat(jnp.exp(draws), extent[dim] // blocks).reshape((-1,) + (1,) * (len(extent) - 1 - dim))
    return factor_of


def noise(rng, dims, width, limit, shards=(), dtype=jnp.bfloat16):
    factor_of = level_of(rng, dims, shards, -0.22, 0.18) if shards else 1.0
    array = jax.random.normal(rng, dims, jnp.float32) * width * factor_of
    return jnp.minimum(jnp.maximum(array, -limit), limit).astype(dtype)


def setup_inputs(seed: int = 0) -> dict:
    key_of = jax.random.split(jax.random.key(seed), 14)
    x_in = draw_x_in(jax.random.fold_in(key_of[13], 71), 0)
    x_new = noise(key_of[1], (SEQS, D), 1.0, 6.0, ((0, 16),))
    w_x = noise(key_of[2], (D, H * P_SIZE), D ** -0.5, 0.125)
    w_b = noise(key_of[3], (D, G * N), D ** -0.5, 0.125)
    w_c = noise(key_of[4], (D, G * N), D ** -0.5, 0.125)
    w_dt = noise(key_of[5], (D, H), D ** -0.5, 0.125)
    w_z = draw_w_z(jax.random.fold_in(key_of[13], 71), 0)
    conv_w = noise(key_of[7], (KW, H * P_SIZE + 2 * G * N), 0.5, 3.0, (), jnp.float32)
    conv_b = noise(key_of[8], (H * P_SIZE + 2 * G * N,), 0.5, 3.0, (), jnp.float32)
    dt_bias = jnp.clip(jax.random.uniform(key_of[9], (H,), jnp.float32, -4.0, -2.0), -4.0, -2.0)
    a_log = draw_a_log(jax.random.fold_in(key_of[13], 71), 0)
    d_skip = jnp.clip(jnp.exp(jax.random.uniform(key_of[11], (H,), jnp.float32, math.log(1.0), math.log(8.0))), 1.0, 8.0)
    norm_g = jnp.clip(1.0 + 0.18 * jax.random.normal(key_of[12], (H, P_SIZE), jnp.float32), 0.1, 1.9)
    return {"x_in": x_in, "x_new": x_new, "w_x": w_x, "w_b": w_b, "w_c": w_c, "w_dt": w_dt, "w_z": w_z, "conv_w": conv_w, "conv_b": conv_b, "dt_bias": dt_bias, "a_log": a_log, "d_skip": d_skip, "norm_g": norm_g}


eps = 1e-05

def shift_conv(padded, weights, biases, col_count):
    acc_sum = biases + jnp.zeros(padded.shape[:1] + (col_count,) + padded.shape[2:], jnp.float32)
    for offset in range(KW):
        acc_sum = acc_sum + weights[offset] * padded[:, offset:offset + col_count].astype(jnp.float32)
    return jax.nn.silu(acc_sum).astype(jnp.bfloat16)

def reference(x_in, x_new, w_x, w_b, w_c, w_dt, w_z, conv_w, conv_b, dt_bias, a_log, d_skip, norm_g):
    inner_cols = H * P_SIZE
    state_cols = G * N
    edge_rows = KW - 1
    decay_rates = -jnp.exp(a_log)

    def one_sequence(token_rows):
        pre_values = jnp.dot(token_rows, w_x, preferred_element_type=jnp.float32).astype(jnp.bfloat16)
        pre_keys = jnp.dot(token_rows, w_b, preferred_element_type=jnp.float32).astype(jnp.bfloat16)
        raw_steps = jnp.dot(token_rows, w_dt, preferred_element_type=jnp.float32).astype(jnp.bfloat16)
        joined = jnp.concatenate([pre_values, pre_keys], axis=1)
        padded = jnp.concatenate([jnp.zeros((edge_rows, joined.shape[1]), jnp.bfloat16), joined], axis=0)
        conved = shift_conv(padded[None], conv_w[:, :inner_cols + state_cols], conv_b[:inner_cols + state_cols], LENGTH)[0]
        step_sizes = jax.nn.softplus(raw_steps.astype(jnp.float32) + dt_bias)
        rest_sum = lax.cumsum(step_sizes, axis=0, reverse=True) - step_sizes
        weight = jnp.exp(decay_rates * rest_sum) * step_sizes
        scaled = (weight[:, :, None] * conved[:, :inner_cols].astype(jnp.float32).reshape(LENGTH, H, P_SIZE)).astype(jnp.bfloat16)
        key_rows = conved[:, inner_cols:].astype(jnp.float32).reshape(LENGTH, G, N)
        state = jnp.einsum('lgrp,lgn->grpn', scaled.astype(jnp.float32).reshape(LENGTH, G, R, P_SIZE), key_rows, precision=lax.Precision.HIGHEST).reshape(H, P_SIZE, N)
        pre_query = jnp.dot(token_rows[LENGTH - edge_rows:], w_c, preferred_element_type=jnp.float32).astype(jnp.bfloat16)
        tail_rows = jnp.concatenate([joined[LENGTH - edge_rows:], pre_query], axis=1)
        return (state, tail_rows)
    states, tails = lax.map(one_sequence, x_in)
    new_pre = jnp.concatenate([jnp.dot(x_new, w_x, preferred_element_type=jnp.float32).astype(jnp.bfloat16), jnp.dot(x_new, w_b, preferred_element_type=jnp.float32).astype(jnp.bfloat16), jnp.dot(x_new, w_c, preferred_element_type=jnp.float32).astype(jnp.bfloat16)], axis=1)
    new_raw = jnp.dot(x_new, w_dt, preferred_element_type=jnp.float32).astype(jnp.bfloat16)
    gate_new = jnp.dot(x_new, w_z, preferred_element_type=jnp.float32).astype(jnp.bfloat16)
    padded = jnp.concatenate([tails, new_pre[:, None, :]], axis=1)
    new_conv = shift_conv(padded, conv_w, conv_b, 1)[:, 0]
    new_values = new_conv[:, :inner_cols].astype(jnp.float32).reshape(SEQS, G, R, P_SIZE)
    new_keys = new_conv[:, inner_cols:inner_cols + state_cols].astype(jnp.float32).reshape(SEQS, G, N)
    new_query = new_conv[:, inner_cols + state_cols:].astype(jnp.float32).reshape(SEQS, G, N)
    new_steps = jax.nn.softplus(new_raw.astype(jnp.float32) + dt_bias)
    decay_new = jnp.exp(decay_rates * new_steps).reshape(SEQS, G, R)
    held_read = jnp.einsum('sgrpn,sgn->sgrp', states.reshape(SEQS, G, R, P_SIZE, N), new_query, precision=lax.Precision.HIGHEST)
    inner_prod = lax.optimization_barrier(jnp.sum(new_query * new_keys, axis=-1))
    step_group = new_steps.reshape(SEQS, G, R)
    output = decay_new[..., None] * held_read + (step_group * inner_prod[:, :, None])[..., None] * new_values + d_skip.reshape(G, R)[None, :, :, None] * new_values
    gated_out = output * jax.nn.silu(gate_new.astype(jnp.float32).reshape(SEQS, G, R, P_SIZE))
    group_ms = lax.optimization_barrier(jnp.mean(gated_out * gated_out, axis=(2, 3)))
    read_out = gated_out * lax.rsqrt(group_ms + eps)[:, :, None, None] * norm_g.reshape(G, R, P_SIZE)
    return (states.astype(jnp.bfloat16), read_out.astype(jnp.bfloat16).reshape(SEQS, H, P_SIZE))
```

```python
import jax
import jax.numpy as jnp
from jax import lax
from jax.experimental import pallas as pl
from jax.experimental.pallas import tpu as pltpu
from jax.sharding import PartitionSpec as P

H = 32
P_SIZE = 64
G = 8
N = 128
KW = 4
R = 4
D = 2048
T = 384
eps = 1e-05
MESH = pl.DeviceIdType.MESH
BF = jnp.bfloat16
F32 = jnp.float32
OFFS = (2, 1, 3, 0)
SP = 16


def dot(a, b):
    return jnp.dot(a, b, preferred_element_type=F32)


def dot_exact(a, b):
    return jnp.dot(a, b, preferred_element_type=F32, precision=lax.Precision.HIGHEST)


def softplus(v):
    return jnp.maximum(v, 0.0) + jnp.log1p(jnp.exp(-jnp.abs(v)))


def kernel(
    x_hbm, xnew_ref, wx_hbm, wb_hbm, wc_hbm, wdt_hbm, wz_hbm,
    cw_ref, cb_ref, dtb_ref, alog_ref, dskip_ref, ng_ref,
    st_out, ro_out,
    x_ref, wx_ref, wb_ref, wc_ref, wdt_ref, wz_ref,
    pre_refs, key_refs, sc_refs, wg_ref, fac_ref,
    edge_tx, halo_rx, tail_rx, tot_tx, tot_rx,
    tx1, rx1, tx2, rx2,
    in_sems, w_sems,
    halo_s, halo_r, tail_s, tail_r, tot_s, tot_r, s1_s, s1_r, s2_s, s2_r,
):
    i = lax.axis_index("sp")
    j = lax.axis_index("tp")
    zp, xp = i // 4, i % 4
    yp, cp = j // 2, j % 2
    other = 1 - cp

    def pair(t):
        return (yp + OFFS[t]) % 4

    x_copies = [
        pltpu.make_async_copy(x_hbm.at[s], x_ref.at[pl.ds(T * s, T), :], in_sems.at[s])
        for s in range(2)
    ]
    wdt_copy = pltpu.make_async_copy(wdt_hbm, wdt_ref, in_sems.at[2])
    wz_copy = pltpu.make_async_copy(wz_hbm, wz_ref, in_sems.at[3])
    wc_copy = pltpu.make_async_copy(
        wc_hbm.at[:, pl.ds(pl.multiple_of(j * N, N), N)], wc_ref, in_sems.at[4]
    )

    def w_copy(t):
        q = pair(t)
        kcols = pl.ds(pl.multiple_of(q * 256, 256), 256)
        vcols = pl.ds(pl.multiple_of(q * 512, 512), 512)
        return [
            pltpu.make_async_copy(wb_hbm.at[:, kcols], wb_ref.at[:, kcols], w_sems.at[t, 0]),
            pltpu.make_async_copy(wx_hbm.at[:, vcols], wx_ref.at[:, vcols], w_sems.at[t, 1]),
        ]

    wdt_copy.start()
    x_copies[0].start()
    x_copies[1].start()
    for t in range(4):
        for c in w_copy(t):
            c.start()
    wz_copy.start()
    wc_copy.start()

    bar = pltpu.get_barrier_semaphore()

    def sig(sp, tp):
        pl.semaphore_signal(bar, inc=1, device_id=(sp, tp), device_id_type=MESH)

    for d in range(1, SP):
        sig((i + d) % SP, j)

    @pl.when(cp != xp // 2)
    def _():
        for d in range(4):
            sig(zp * 4 + d, 2 * yp + other)

    for d in range(4):
        @pl.when((d != zp) | (yp != zp))
        def _():
            sig(d * 4 + xp, 2 * zp + cp)

    tail_tp = i // 2

    @pl.when((i != SP - 1) | (j != tail_tp))
    def _():
        sig(SP - 1, tail_tp)

    wdt_copy.wait()
    x_copies[0].wait()
    x_copies[1].wait()
    lo = x_ref[T - 16:T, :].astype(F32)[13:16]
    hi = x_ref[2 * T - 16:2 * T, :].astype(F32)[13:16]
    edge_tx[...] = jnp.concatenate([lo, hi, jnp.zeros((2, D), F32)], axis=0).astype(BF)
    raw = dot(x_ref[0:2 * T, :], wdt_ref[...])
    steps = softplus(raw + dtb_ref[...])
    tot_tx[...] = jnp.zeros_like(tot_tx)
    rates = -jnp.exp(alog_ref[...])
    upper = (
        lax.broadcasted_iota(jnp.int32, (T, T), 1) > lax.broadcasted_iota(jnp.int32, (T, T), 0)
    ).astype(F32).astype(BF)
    for s in range(2):
        own = steps[T * s:T * (s + 1)]
        tot_tx[s:s + 1, 0:H] = jnp.sum(own, axis=0, keepdims=True)
        high = own.astype(BF)
        low = (own - high.astype(F32)).astype(BF)
        rest = dot(upper, high) + dot(upper, low)
        weight = jnp.exp(rates * rest) * own
        for g in range(G):
            wg_ref[g, T * s:T * (s + 1), 0:R] = weight[:, R * g:R * (g + 1)]

    def w_slices(t):
        q = pair(t)
        return [
            wb_ref[:, pl.ds(pl.multiple_of(q * 256, 256), 256)],
            wx_ref[:, pl.ds(pl.multiple_of(q * 512, 256), 256)],
            wx_ref[:, pl.ds(pl.multiple_of(q * 512 + 256, 256), 256)],
        ]

    def put_halo(pre, rows):
        for c in range(2):
            pre[c, 5:8, :] = rows[0:3, 128 * c:128 * (c + 1)]
            pre[c, T + 13:T + 16, :] = rows[3:6, 128 * c:128 * (c + 1)]

    def proj(pre, w, s, halo):
        rows = T + (16 if halo and s == 1 else 0)
        res = dot(x_ref[T * s:T * s + rows, :], w)
        for c in range(2):
            pre[c, (T + 8) * s + 8:(T + 8) * (s + 1), :] = res[0:T, 128 * c:128 * (c + 1)]
        if halo and s == 1:
            put_halo(pre, res[T:T + 8])

    for c in w_copy(0):
        c.wait()
    for u, w in enumerate(w_slices(0)):
        for s in range(2):
            proj(pre_refs[u], w, s, False)

    s1_self = (cp == xp // 2)
    arrivals = 15 + 2 + 4 - jnp.where(zp == yp, 1, 0)
    arrivals = arrivals + jnp.where(i == SP - 1, 16 - jnp.where(j == 7, 1, 0), 0)
    pl.semaphore_wait(bar, arrivals)

    halo_copy = pltpu.make_async_remote_copy(
        edge_tx, halo_rx, halo_s, halo_r, device_id=((i + 1) % SP, j), device_id_type=MESH
    )
    halo_copy.start()

    def tot_copy(d):
        return pltpu.make_async_remote_copy(
            tot_tx, tot_rx.at[i], tot_s.at[d], tot_r.at[i],
            device_id=((i + d) % SP, j), device_id_type=MESH,
        )

    for d in range(1, SP):
        tot_copy(d).start()

    def tail_copy(n):
        return pltpu.make_async_remote_copy(
            edge_tx, tail_rx, tail_s.at[n], tail_r,
            device_id=(2 * j + n % 2, n // 2), device_id_type=MESH,
        )

    def tail_self(n):
        return (j == 7) & (2 * j + n % 2 == i) & (n // 2 == j)

    @pl.when(i == SP - 1)
    def _():
        for n in range(16):
            @pl.when(jnp.logical_not(tail_self(n)))
            def _():
                tail_copy(n).start()

    @pl.when((i == SP - 1) & (j == 7))
    def _():
        tail_rx[...] = edge_tx[...]

    halo_copy.wait_recv()
    keep = jnp.where(i > 0, 1.0, 0.0).astype(F32)
    halo = jnp.where(i > 0, halo_rx[...].astype(F32), 0.0)
    x_ref[2 * T:2 * T + 16, :] = jnp.concatenate([halo, jnp.zeros((8, D), F32)], axis=0).astype(BF)
    for u, w in enumerate(w_slices(0)):
        put_halo(pre_refs[u], dot(x_ref[2 * T:2 * T + 16, :], w)[0:8])

    for d in range(1, SP):
        src = (i + SP - d) % SP
        pltpu.make_async_remote_copy(
            tot_tx, tot_rx.at[src], tot_s.at[d], tot_r.at[src],
            device_id=((i + d) % SP, j), device_id_type=MESH,
        ).wait_recv()
    later = jnp.zeros((2, 128), F32)
    for d in range(SP):
        later = later + jnp.where(i < d, tot_rx[d], 0.0)
    factor = jnp.exp(rates * later[:, 0:H])
    spread = (
        lax.broadcasted_iota(jnp.int32, (H, H * P_SIZE), 1) // P_SIZE
        == lax.broadcasted_iota(jnp.int32, (H, H * P_SIZE), 0)
    ).astype(F32)
    wide = dot_exact(jnp.concatenate([factor, jnp.zeros((6, H), F32)], axis=0), spread)
    for g in range(G):
        fac_ref[g] = wide[:, 256 * g:256 * (g + 1)]

    lane = lax.broadcasted_iota(jnp.int32, (128, 128), 1)

    def conv(pre, s, c, r, off):
        cols = pl.ds(pl.multiple_of(off + 128 * c, 128), 128)
        taps = cw_ref[:, cols] * 0.5
        acc = cb_ref[:, cols] * 0.5 + taps[3:4] * pre[c, pl.ds((T + 8) * s + 8 + r, 128), :]
        for k in range(3):
            acc = acc + taps[k:k + 1] * pre[c, pl.ds((T + 8) * s + 5 + k + r, 128), :]
        return acc + acc * jnp.tanh(acc)

    def post_keys(t, s):
        q = pair(t)
        for c in range(2):
            for r in range(0, T, 128):
                out = conv(pre_refs[3 * (t % 2)], s, c, r, H * P_SIZE + q * 256)
                key_refs[t % 2][T * s + r:T * s + r + 128, 128 * c:128 * (c + 1)] = out.astype(BF)

    def post_values(t, b, s):
        g = 2 * pair(t) + b
        for c in range(2):
            for r in range(0, T, 128):
                out = conv(pre_refs[3 * (t % 2) + 1 + b], s, c, r, g * 256)
                w = wg_ref[g, pl.ds(T * s + r, 128), 0:R]
                w = jnp.where(lane < P_SIZE, w[:, 2 * c:2 * c + 1], w[:, 2 * c + 1:2 * c + 2])
                sc_refs[b][T * s + r:T * s + r + 128, 128 * c:128 * (c + 1)] = (out * w).astype(BF)

    def s1_copy(t, a, b):
        n = 4 * t + 2 * a + b
        return pltpu.make_async_remote_copy(
            tx1.at[n], rx1.at[t, xp], s1_s.at[n], s1_r.at[t, xp],
            device_id=(zp * 4 + 2 * cp + a, 2 * yp + b), device_id_type=MESH,
        )

    def s1_own(a, b):
        return (xp == 2 * cp + a) & (cp == b)

    def contract(t, a, b):
        g = 2 * pair(t) + b
        keys = key_refs[t % 2][T * a:T * (a + 1), 128 * b:128 * (b + 1)]
        term = lax.dot_general(
            keys, sc_refs[b][T * a:T * (a + 1), :], (((0,), (0,)), ((), ())),
            preferred_element_type=F32,
        )
        term = term * fac_ref[g, a:a + 1, :]
        tx1[4 * t + 2 * a + b] = term.astype(BF)

    def send1(t, a, b):
        @pl.when(jnp.logical_not(s1_own(a, b)))
        def _():
            s1_copy(t, a, b).start()

        @pl.when(s1_own(a, b))
        def _():
            rx1[t, xp] = tx1[4 * t + 2 * a + b]

    def s2_copy(t):
        return pltpu.make_async_remote_copy(
            tx2.at[t], rx2.at[zp], s2_s.at[t], s2_r.at[zp],
            device_id=(yp * 4 + xp, 2 * pair(t) + cp), device_id_type=MESH,
        )

    def s2_self(t):
        return (yp == zp) if OFFS[t] == 0 else None

    def stage2(t):
        for d in range(4):
            @pl.when(jnp.logical_not((d == xp) & s1_self))
            def _():
                pltpu.make_async_remote_copy(
                    tx1.at[0], rx1.at[t, d], s1_s.at[0], s1_r.at[t, d],
                    device_id=(i, j), device_id_type=MESH,
                ).wait_recv()
        acc = rx1[t, 0].astype(F32)
        for d in range(1, 4):
            acc = acc + rx1[t, d].astype(F32)
        tx2[t] = acc.astype(BF)
        if OFFS[t] == 0:
            @pl.when(yp != zp)
            def _():
                s2_copy(t).start()

            @pl.when(yp == zp)
            def _():
                rx2[zp] = tx2[t]
        else:
            s2_copy(t).start()

    for t in range(4):
        nxt = t + 1
        if nxt < 4:
            for c in w_copy(nxt):
                c.wait()
            ws = w_slices(nxt)
        for s in range(2):
            if nxt < 4:
                proj(pre_refs[3 * (nxt % 2)], ws[0], s, True)
            post_keys(t, s)
        for b in range(2):
            for s in range(2):
                if nxt < 4:
                    proj(pre_refs[3 * (nxt % 2) + 1 + b], ws[1 + b], s, True)
                post_values(t, b, s)
                contract(t, s, b)
        for b in range(2):
            for a in range(2):
                send1(t, a, b)
        if t > 0:
            stage2(t - 1)

    wz_copy.wait()
    wc_copy.wait()

    @pl.when(jnp.logical_not((i == SP - 1) & (j == 7)))
    def _():
        tail_copy(0).wait_recv()

    ext = jnp.concatenate(
        [tail_rx[...].astype(F32), jnp.broadcast_to(xnew_ref[...].astype(F32), (8, D))], axis=0
    ).astype(BF)
    a_own = i % 2

    def fresh(w, off, width):
        res = dot(ext, w)
        cols = pl.ds(pl.multiple_of(off, 128), width)
        taps = cw_ref[:, cols] * 0.5
        acc = cb_ref[:, cols] * 0.5 + taps[3:4] * res[8:9]
        for k in range(3):
            acc = acc + taps[k:k + 1] * jnp.where(a_own == 0, res[k:k + 1], res[3 + k:4 + k])
        return acc + acc * jnp.tanh(acc)

    values = fresh(wx_ref[:, pl.ds(pl.multiple_of(j * 256, 256), 256)], j * 256, 256)
    keys = fresh(wb_ref[:, pl.ds(pl.multiple_of(j * N, N), N)], H * P_SIZE + j * N, N)
    query = fresh(wc_ref[...], H * P_SIZE + G * N + j * N, N)
    gate = dot(ext, wz_ref[...])[8:9]
    new_raw = dot(ext, wdt_ref[...])[8:9]
    new_steps = softplus(new_raw + dtb_ref[...])
    row = lax.broadcasted_iota(jnp.int32, (8, H), 0)
    packed = jnp.where(
        row == 0, new_steps, jnp.where(row == 1, jnp.exp(rates * new_steps), dskip_ref[...])
    )
    own_spread = (
        lax.broadcasted_iota(jnp.int32, (H, 256), 1) // P_SIZE + R * j
        == lax.broadcasted_iota(jnp.int32, (H, 256), 0)
    ).astype(F32)
    per_lane = dot_exact(packed, own_spread)
    step_row, decay_row, skip_row = per_lane[0:1], per_lane[1:2], per_lane[2:3]
    inner = jnp.sum(query * keys, axis=1, keepdims=True)
    direct = (step_row * inner + skip_row) * values
    gate = gate * jax.nn.sigmoid(gate)

    stage2(3)

    for d in range(4):
        @pl.when(jnp.logical_not((d == zp) & (yp == zp)))
        def _():
            pltpu.make_async_remote_copy(
                tx2.at[0], rx2.at[d], s2_s.at[0], s2_r.at[d],
                device_id=(i, j), device_id_type=MESH,
            ).wait_recv()
    state = rx2[0].astype(F32)
    for d in range(1, 4):
        state = state + rx2[d].astype(F32)
    st_out[0] = state.T.astype(BF).reshape(R, P_SIZE, N)
    held = dot_exact(jnp.broadcast_to(query, (8, N)), state)[0:1]
    gated = (decay_row * held + direct) * gate
    ms = jnp.sum(gated * gated, axis=1, keepdims=True) * (1.0 / 256)
    normed = gated * lax.rsqrt(ms + eps)
    head = lax.broadcasted_iota(jnp.int32, (R, 256), 0)
    chan = lax.broadcasted_iota(jnp.int32, (R, 256), 1) // P_SIZE
    split = jnp.where(head == chan, normed, 0.0)
    split = split[:, 0:128] + split[:, 128:256]
    split = split[:, 0:P_SIZE] + split[:, P_SIZE:128]
    ro_out[0] = (split * ng_ref[...]).astype(BF)

    halo_copy.wait_send()
    for d in range(1, SP):
        tot_copy(d).wait_send()

    @pl.when(i == SP - 1)
    def _():
        for n in range(16):
            @pl.when(jnp.logical_not(tail_self(n)))
            def _():
                tail_copy(n).wait_send()

    for t in range(4):
        for a in range(2):
            for b in range(2):
                @pl.when(jnp.logical_not(s1_own(a, b)))
                def _():
                    s1_copy(t, a, b).wait_send()
        if OFFS[t] == 0:
            @pl.when(yp != zp)
            def _():
                s2_copy(t).wait_send()
        else:
            s2_copy(t).wait_send()


def per_device(
    x_in, x_new, w_x, w_b, w_c, w_dt, w_z, conv_w, conv_b, dt_bias, a_log, d_skip, norm_g
):
    hbm = pl.BlockSpec(memory_space=pl.ANY)
    vmem = pl.BlockSpec(memory_space=pltpu.VMEM)
    dma = pltpu.SemaphoreType.DMA
    return pl.pallas_call(
        kernel,
        out_shape=(
            jax.ShapeDtypeStruct((1, R, P_SIZE, N), BF),
            jax.ShapeDtypeStruct((1, R, P_SIZE), BF),
        ),
        in_specs=[hbm, vmem, hbm, hbm, hbm, hbm, hbm] + [vmem] * 6,
        out_specs=(vmem, vmem),
        scratch_shapes=[
            pltpu.VMEM((2 * T + 16, D), BF),
            pltpu.VMEM((D, H * P_SIZE), BF),
            pltpu.VMEM((D, G * N), BF),
            pltpu.VMEM((D, N), BF),
            pltpu.VMEM((D, H), BF),
            pltpu.VMEM((D, 256), BF),
            [pltpu.VMEM((2, 2 * (T + 8), 128), F32) for _ in range(6)],
            [pltpu.VMEM((2 * T, 256), BF) for _ in range(2)],
            [pltpu.VMEM((2 * T, 256), BF) for _ in range(2)],
            pltpu.VMEM((G, 2 * T, 128), F32),
            pltpu.VMEM((G, 8, 256), F32),
            pltpu.VMEM((8, D), BF),
            pltpu.VMEM((8, D), BF),
            pltpu.VMEM((8, D), BF),
            pltpu.VMEM((2, 128), F32),
            pltpu.VMEM((SP, 2, 128), F32),
            pltpu.VMEM((16, N, 256), BF),
            pltpu.VMEM((4, 4, N, 256), BF),
            pltpu.VMEM((4, N, 256), BF),
            pltpu.VMEM((4, N, 256), BF),
            dma((5,)),
            dma((4, 2)),
            dma,
            dma,
            dma((16,)),
            dma,
            dma((SP,)),
            dma((SP,)),
            dma((16,)),
            dma((4, 4)),
            dma((4,)),
            dma((4,)),
        ],
        compiler_params=pltpu.CompilerParams(
            collective_id=0, has_side_effects=True, vmem_limit_bytes=60 * 1024 * 1024
        ),
    )(
        x_in, x_new, w_x, w_b, w_c, w_dt, w_z, conv_w,
        conv_b.reshape(1, -1), dt_bias.reshape(1, -1), a_log.reshape(1, -1),
        d_skip.reshape(1, -1), norm_g,
    )


def solution(mesh):
    return jax.shard_map(
        per_device,
        mesh=mesh,
        in_specs=(
            P("tp", "sp", None),
            P("sp", None),
            P(),
            P(),
            P(),
            P(),
            P(None, "tp"),
            P(),
            P(),
            P(),
            P(),
            P(),
            P("tp", None),
        ),
        out_specs=(P("sp", "tp", None, None), P("sp", "tp", None)),
        check_vma=False,
    )
```

```python
import jax
import jax.numpy as jnp
from jax import lax
from jax.experimental import pallas as pl
from jax.experimental.pallas import tpu as pltpu
from jax.sharding import PartitionSpec as P

H = 32
P_SIZE = 64
G = 8
N = 128
KW = 4
R = 4
D = 2048
T = 384
eps = 1e-05
MESH = pl.DeviceIdType.MESH
BF = jnp.bfloat16
F32 = jnp.float32
OFFS = (2, 1, 3, 0)
SP = 16


def dot(a, b):
    return jnp.dot(a, b, preferred_element_type=F32)


def dot_t(a, b):
    return lax.dot_general(a, b, (((1,), (1,)), ((), ())), preferred_element_type=F32)


def dot_exact(a, b):
    return jnp.dot(a, b, preferred_element_type=F32, precision=lax.Precision.HIGHEST)


def softplus(v):
    return jnp.maximum(v, 0.0) + jnp.log1p(jnp.exp(-jnp.abs(v)))


def kernel(
    x_hbm, xnew_hbm, wx_hbm, wb_hbm, wc_hbm, wdt_hbm, wz_hbm,
    cw_hbm, cb_hbm, dtb_hbm, alog_hbm, dskip_hbm, ng_hbm,
    st_out, ro_out,
    x_ref, xnew_ref, wx_ref, wb_ref, wc_ref, wdt_ref, wz_ref,
    cw_ref, cb_ref, dtb_ref, alog_ref, dskip_ref, ng_ref,
    pre_refs, key_refs, sc_refs, wg_ref, fac_ref,
    edge_tx, halo_rx, tail_rx, tot_tx, tot_rx,
    tx1, rx1, tx2, rx2,
    in_sems, w_sems,
    halo_s, halo_r, tail_s, tail_r, tot_s, tot_r, s1_s, s1_r, s2_s, s2_r,
):
    scope = jax.named_scope
    i = lax.axis_index("sp")
    j = lax.axis_index("tp")
    zp, xp = i // 4, i % 4
    yp, cp = j // 2, j % 2
    other = 1 - cp

    def pair(t):
        return (yp + OFFS[t]) % 4

    def load(src, dst, n):
        return pltpu.make_async_copy(src, dst, in_sems.at[n])

    first_loads = [
        load(x_hbm.at[0], x_ref.at[pl.ds(0, T), :], 0),
        load(x_hbm.at[1], x_ref.at[pl.ds(T, T), :], 1),
        load(wdt_hbm, wdt_ref, 2),
        load(dtb_hbm, dtb_ref, 3),
        load(alog_hbm, alog_ref, 4),
    ]
    conv_loads = [load(cw_hbm, cw_ref, 5), load(cb_hbm, cb_ref, 6)]
    last_loads = [
        load(xnew_hbm, xnew_ref, 7),
        load(dskip_hbm, dskip_ref, 8),
        load(ng_hbm, ng_ref, 9),
        load(wz_hbm, wz_ref, 10),
        load(wc_hbm.at[:, pl.ds(pl.multiple_of(j * N, N), N)], wc_ref, 11),
    ]

    def w_copy(t):
        q = pair(t)
        kcols = pl.ds(pl.multiple_of(q * 256, 256), 256)
        vcols = pl.ds(pl.multiple_of(q * 512, 512), 512)
        return [
            pltpu.make_async_copy(wb_hbm.at[:, kcols], wb_ref.at[:, kcols], w_sems.at[t, 0]),
            pltpu.make_async_copy(wx_hbm.at[:, vcols], wx_ref.at[:, vcols], w_sems.at[t, 1]),
        ]

    for c in first_loads + w_copy(0):
        c.start()

    bar = pltpu.get_barrier_semaphore()

    def sig(sp, tp):
        pl.semaphore_signal(bar, inc=1, device_id=(sp, tp), device_id_type=MESH)

    for d in range(1, SP):
        sig((i + d) % SP, j)

    @pl.when(cp != xp // 2)
    def _():
        for d in range(4):
            sig(zp * 4 + d, 2 * yp + other)

    for d in range(4):
        @pl.when((d != zp) | (yp != zp))
        def _():
            sig(d * 4 + xp, 2 * zp + cp)

    tail_tp = i // 2

    @pl.when((i != SP - 1) | (j != tail_tp))
    def _():
        sig(SP - 1, tail_tp)

    for c in conv_loads:
        c.start()

    with scope("xwait"):
        for c in first_loads:
            c.wait()
    for t in range(1, 4):
        for c in w_copy(t):
            c.start()
    for c in last_loads:
        c.start()
    lo = x_ref[T - 16:T, :].astype(F32)[13:16]
    hi = x_ref[2 * T - 16:2 * T, :].astype(F32)[13:16]
    edge_tx[...] = jnp.concatenate([lo, hi, jnp.zeros((2, D), F32)], axis=0).astype(BF)

    raw = dot_t(x_ref[0:2 * T, :], wdt_ref[...])
    steps = softplus(raw + dtb_ref[...])
    tot_tx[...] = jnp.zeros_like(tot_tx)
    rates = -jnp.exp(alog_ref[...])
    for s in range(2):
        tot_tx[s:s + 1, 0:H] = jnp.sum(steps[T * s:T * (s + 1)], axis=0, keepdims=True)

    s1_self = (cp == xp // 2)
    arrivals = 15 + 2 + 4 - jnp.where(zp == yp, 1, 0)
    arrivals = arrivals + jnp.where(i == SP - 1, 16 - jnp.where(j == 7, 1, 0), 0)
    with scope("barrier"):
        pl.semaphore_wait(bar, arrivals)

    halo_copy = pltpu.make_async_remote_copy(
        edge_tx, halo_rx, halo_s, halo_r, device_id=((i + 1) % SP, j), device_id_type=MESH
    )

    @pl.when(i < SP - 1)
    def _():
        halo_copy.start()

    def tot_copy(d):
        return pltpu.make_async_remote_copy(
            tot_tx, tot_rx.at[i], tot_s.at[d], tot_r.at[i],
            device_id=((i + d) % SP, j), device_id_type=MESH,
        )

    for d in range(1, SP):
        tot_copy(d).start()

    with scope("w0wait"):
        for c in w_copy(0):
            c.wait()
        for c in conv_loads:
            c.wait()

    upper = (
        lax.broadcasted_iota(jnp.int32, (T, T), 1) > lax.broadcasted_iota(jnp.int32, (T, T), 0)
    ).astype(F32).astype(BF)

    def weights(s):
        own = steps[T * s:T * (s + 1)]
        high = own.astype(BF)
        low = (own - high.astype(F32)).astype(BF)
        rest = dot(upper, high) + dot(upper, low)
        weight = jnp.exp(rates * rest) * own
        for g in range(G):
            wg_ref[g, T * s:T * (s + 1), 0:R] = weight[:, R * g:R * (g + 1)]

    def w_slice(t, u):
        q = pair(t)
        if u == 0:
            return wb_ref[:, pl.ds(pl.multiple_of(q * 256, 256), 256)]
        return wx_ref[:, pl.ds(pl.multiple_of(q * 512 + 256 * (u - 1), 256), 256)]

    def put_halo(pre, rows):
        for c in range(2):
            pre[c, 5:8, :] = rows[0:3, 128 * c:128 * (c + 1)]
            pre[c, T + 13:T + 16, :] = rows[3:6, 128 * c:128 * (c + 1)]

    def pre_of(n):
        return pre_refs[n % 6]

    def proj(n, s):
        t, u = n // 3, n % 3
        pre = pre_of(n)
        rows = T + (16 if t > 0 and s == 1 else 0)
        res = dot(x_ref[T * s:T * s + rows, :], w_slice(t, u))
        for c in range(2):
            pre[c, (T + 8) * s + 8:(T + 8) * (s + 1), :] = res[0:T, 128 * c:128 * (c + 1)]
        if t > 0 and s == 1:
            put_halo(pre, res[T:T + 8])

    for n in range(3):
        for s in range(2):
            proj(n, s)
            if n == 1:
                weights(s)

    with scope("halowait"):
        @pl.when(i > 0)
        def _():
            halo_copy.wait_recv()
    halo = jnp.where(i > 0, halo_rx[...].astype(F32), 0.0)
    x_ref[2 * T:2 * T + 16, :] = jnp.concatenate([halo, jnp.zeros((8, D), F32)], axis=0).astype(BF)
    for u in range(3):
        put_halo(pre_of(u), dot(x_ref[2 * T:2 * T + 16, :], w_slice(0, u))[0:8])

    lane = lax.broadcasted_iota(jnp.int32, (128, 128), 1)

    def conv(pre, s, c, r, off):
        cols = pl.ds(pl.multiple_of(off + 128 * c, 128), 128)
        taps = cw_ref[:, cols] * 0.5
        acc = cb_ref[:, cols] * 0.5 + taps[3:4] * pre[c, pl.ds((T + 8) * s + 8 + r, 128), :]
        for k in range(3):
            acc = acc + taps[k:k + 1] * pre[c, pl.ds((T + 8) * s + 5 + k + r, 128), :]
        return acc + acc * jnp.tanh(acc)

    def post_keys(t, s):
        q = pair(t)
        for c in range(2):
            for r in range(0, T, 128):
                out = conv(pre_of(3 * t), s, c, r, H * P_SIZE + q * 256)
                key_refs[t % 2][T * s + r:T * s + r + 128, 128 * c:128 * (c + 1)] = out.astype(BF)

    def post_values(t, b, s):
        g = 2 * pair(t) + b
        for c in range(2):
            for r in range(0, T, 128):
                out = conv(pre_of(3 * t + 1 + b), s, c, r, g * 256)
                w = wg_ref[g, pl.ds(T * s + r, 128), 0:R]
                w = jnp.where(lane < P_SIZE, w[:, 2 * c:2 * c + 1], w[:, 2 * c + 1:2 * c + 2])
                sc_refs[b][T * s + r:T * s + r + 128, 128 * c:128 * (c + 1)] = (out * w).astype(BF)

    def post(n, s):
        if n % 3 == 0:
            post_keys(n // 3, s)
        else:
            post_values(n // 3, n % 3 - 1, s)

    def s1_copy(t, a, b):
        n = 4 * t + 2 * a + b
        return pltpu.make_async_remote_copy(
            tx1.at[n], rx1.at[t, xp], s1_s.at[n], s1_r.at[t, xp],
            device_id=(zp * 4 + 2 * cp + a, 2 * yp + b), device_id_type=MESH,
        )

    def s1_own(a, b):
        return (xp == 2 * cp + a) & (cp == b)

    def contract(t, a, b):
        g = 2 * pair(t) + b
        keys = key_refs[t % 2][T * a:T * (a + 1), 128 * b:128 * (b + 1)]
        term = lax.dot_general(
            keys, sc_refs[b][T * a:T * (a + 1), :], (((0,), (0,)), ((), ())),
            preferred_element_type=F32,
        )
        term = term * fac_ref[g, a:a + 1, :]
        tx1[4 * t + 2 * a + b] = term.astype(BF)

    def send1(t, a, b):
        @pl.when(jnp.logical_not(s1_own(a, b)))
        def _():
            s1_copy(t, a, b).start()

        @pl.when(s1_own(a, b))
        def _():
            rx1[t, xp] = tx1[4 * t + 2 * a + b]

    def s2_copy(t):
        return pltpu.make_async_remote_copy(
            tx2.at[t], rx2.at[zp], s2_s.at[t], s2_r.at[zp],
            device_id=(yp * 4 + xp, 2 * pair(t) + cp), device_id_type=MESH,
        )

    def stage2(t):
        with scope("s1wait"):
            for d in range(4):
                @pl.when(jnp.logical_not((d == xp) & s1_self))
                def _():
                    pltpu.make_async_remote_copy(
                        tx1.at[0], rx1.at[t, d], s1_s.at[0], s1_r.at[t, d],
                        device_id=(i, j), device_id_type=MESH,
                    ).wait_recv()
        acc = rx1[t, 0].astype(F32)
        for d in range(1, 4):
            acc = acc + rx1[t, d].astype(F32)
        tx2[t] = acc.astype(BF)
        if OFFS[t] == 0:
            @pl.when(yp != zp)
            def _():
                s2_copy(t).start()

            @pl.when(yp == zp)
            def _():
                rx2[zp] = tx2[t]
        else:
            s2_copy(t).start()

    def factors():
        with scope("totwait"):
            for d in range(1, SP):
                src = (i + SP - d) % SP
                pltpu.make_async_remote_copy(
                    tot_tx, tot_rx.at[src], tot_s.at[d], tot_r.at[src],
                    device_id=((i + d) % SP, j), device_id_type=MESH,
                ).wait_recv()
        later = jnp.zeros((2, 128), F32)
        for d in range(SP):
            later = later + jnp.where(i < d, tot_rx[d], 0.0)
        factor = jnp.exp(rates * later[:, 0:H])
        spread = (
            lax.broadcasted_iota(jnp.int32, (H, H * P_SIZE), 1) // P_SIZE
            == lax.broadcasted_iota(jnp.int32, (H, H * P_SIZE), 0)
        ).astype(F32)
        wide = dot_exact(jnp.concatenate([factor, jnp.zeros((6, H), F32)], axis=0), spread)
        for g in range(G):
            fac_ref[g] = wide[:, 256 * g:256 * (g + 1)]

    def tail_copy(n):
        return pltpu.make_async_remote_copy(
            edge_tx, tail_rx, tail_s.at[n], tail_r,
            device_id=(2 * j + n % 2, n // 2), device_id_type=MESH,
        )

    def tail_self(n):
        return (j == 7) & (2 * j + n % 2 == i) & (n // 2 == j)

    def send_tails():
        @pl.when(i == SP - 1)
        def _():
            for n in range(16):
                @pl.when(jnp.logical_not(tail_self(n)))
                def _():
                    tail_copy(n).start()

        @pl.when((i == SP - 1) & (j == 7))
        def _():
            tail_rx[...] = edge_tx[...]

    slots = (
        (3, (0,)), (4, (1,)), (5, (2,)), (6, (3,)), (7, (4,)), (8, (5, 6)),
        (9, (7,)), (10, (8, 9)), (11, (10,)), (None, (11,)),
    )
    for k, (p, posts) in enumerate(slots):
        if p is not None and p % 3 == 0:
            with scope("wwait"):
                for c in w_copy(p // 3):
                    c.wait()
        with scope("slot"):
            for s in range(2):
                if p is not None:
                    proj(p, s)
                for n in posts:
                    post(n, s)
        if k == 1:
            factors()
        for n in posts:
            if n % 3:
                t, b = n // 3, n % 3 - 1
                for a in range(2):
                    contract(t, a, b)
                for a in range(2):
                    send1(t, a, b)
        if k == 3:
            send_tails()
        if k == 6:
            stage2(0)
        if k == 8:
            stage2(1)

    with scope("tailwait"):
        for c in last_loads:
            c.wait()

        @pl.when(jnp.logical_not((i == SP - 1) & (j == 7)))
        def _():
            tail_copy(0).wait_recv()

    ext = jnp.concatenate(
        [tail_rx[...].astype(F32), jnp.broadcast_to(xnew_ref[...].astype(F32), (8, D))], axis=0
    ).astype(BF)
    a_own = i % 2

    def fresh(w, off, width):
        res = dot(ext, w)
        cols = pl.ds(pl.multiple_of(off, 128), width)
        taps = cw_ref[:, cols] * 0.5
        acc = cb_ref[:, cols] * 0.5 + taps[3:4] * res[8:9]
        for k in range(3):
            acc = acc + taps[k:k + 1] * jnp.where(a_own == 0, res[k:k + 1], res[3 + k:4 + k])
        return acc + acc * jnp.tanh(acc)

    values = fresh(wx_ref[:, pl.ds(pl.multiple_of(j * 256, 256), 256)], j * 256, 256)
    keys = fresh(wb_ref[:, pl.ds(pl.multiple_of(j * N, N), N)], H * P_SIZE + j * N, N)
    query = fresh(wc_ref[...], H * P_SIZE + G * N + j * N, N)
    gate = dot(ext, wz_ref[...])[8:9]
    new_raw = dot_t(ext, wdt_ref[...])[8:9]
    new_steps = softplus(new_raw + dtb_ref[...])
    row = lax.broadcasted_iota(jnp.int32, (8, H), 0)
    packed = jnp.where(
        row == 0, new_steps, jnp.where(row == 1, jnp.exp(rates * new_steps), dskip_ref[...])
    )
    own_spread = (
        lax.broadcasted_iota(jnp.int32, (H, 256), 1) // P_SIZE + R * j
        == lax.broadcasted_iota(jnp.int32, (H, 256), 0)
    ).astype(F32)
    per_lane = dot_exact(packed, own_spread)
    step_row, decay_row, skip_row = per_lane[0:1], per_lane[1:2], per_lane[2:3]
    inner = jnp.sum(query * keys, axis=1, keepdims=True)
    direct = (step_row * inner + skip_row) * values
    gate = gate * jax.nn.sigmoid(gate)

    stage2(2)
    stage2(3)

    with scope("s2wait"):
        for d in range(4):
            @pl.when(jnp.logical_not((d == zp) & (yp == zp)))
            def _():
                pltpu.make_async_remote_copy(
                    tx2.at[0], rx2.at[d], s2_s.at[0], s2_r.at[d],
                    device_id=(i, j), device_id_type=MESH,
                ).wait_recv()
    state = rx2[0].astype(F32)
    for d in range(1, 4):
        state = state + rx2[d].astype(F32)
    st_out[0] = state.T.astype(BF).reshape(R, P_SIZE, N)
    held = dot_exact(jnp.broadcast_to(query, (8, N)), state)[0:1]
    gated = (decay_row * held + direct) * gate
    ms = jnp.sum(gated * gated, axis=1, keepdims=True) * (1.0 / 256)
    normed = gated * lax.rsqrt(ms + eps)
    head = lax.broadcasted_iota(jnp.int32, (R, 256), 0)
    chan = lax.broadcasted_iota(jnp.int32, (R, 256), 1) // P_SIZE
    split = jnp.where(head == chan, normed, 0.0)
    split = split[:, 0:128] + split[:, 128:256]
    split = split[:, 0:P_SIZE] + split[:, P_SIZE:128]
    ro_out[0] = (split * ng_ref[...]).astype(BF)

    with scope("drain"):
        @pl.when(i < SP - 1)
        def _():
            halo_copy.wait_send()

        for d in range(1, SP):
            tot_copy(d).wait_send()

        @pl.when(i == SP - 1)
        def _():
            for n in range(16):
                @pl.when(jnp.logical_not(tail_self(n)))
                def _():
                    tail_copy(n).wait_send()

        for t in range(4):
            for a in range(2):
                for b in range(2):
                    @pl.when(jnp.logical_not(s1_own(a, b)))
                    def _():
                        s1_copy(t, a, b).wait_send()
            if OFFS[t] == 0:
                @pl.when(yp != zp)
                def _():
                    s2_copy(t).wait_send()
            else:
                s2_copy(t).wait_send()


def per_device(
    x_in, x_new, w_x, w_b, w_c, w_dt, w_z, conv_w, conv_b, dt_bias, a_log, d_skip, norm_g
):
    hbm = pl.BlockSpec(memory_space=pl.ANY)
    vmem = pl.BlockSpec(memory_space=pltpu.VMEM)
    dma = pltpu.SemaphoreType.DMA
    return pl.pallas_call(
        kernel,
        out_shape=(
            jax.ShapeDtypeStruct((1, R, P_SIZE, N), BF),
            jax.ShapeDtypeStruct((1, R, P_SIZE), BF),
        ),
        in_specs=[hbm] * 13,
        out_specs=(vmem, vmem),
        scratch_shapes=[
            pltpu.VMEM((2 * T + 16, D), BF),
            pltpu.VMEM((1, D), BF),
            pltpu.VMEM((D, H * P_SIZE), BF),
            pltpu.VMEM((D, G * N), BF),
            pltpu.VMEM((D, N), BF),
            pltpu.VMEM((H, D), BF),
            pltpu.VMEM((D, 256), BF),
            pltpu.VMEM((KW, 4096), F32),
            pltpu.VMEM((1, 4096), F32),
            pltpu.VMEM((1, H), F32),
            pltpu.VMEM((1, H), F32),
            pltpu.VMEM((1, H), F32),
            pltpu.VMEM((R, P_SIZE), F32),
            [pltpu.VMEM((2, 2 * (T + 8), 128), F32) for _ in range(6)],
            [pltpu.VMEM((2 * T, 256), BF) for _ in range(2)],
            [pltpu.VMEM((2 * T, 256), BF) for _ in range(2)],
            pltpu.VMEM((G, 2 * T, 128), F32),
            pltpu.VMEM((G, 8, 256), F32),
            pltpu.VMEM((8, D), BF),
            pltpu.VMEM((8, D), BF),
            pltpu.VMEM((8, D), BF),
            pltpu.VMEM((2, 128), F32),
            pltpu.VMEM((SP, 2, 128), F32),
            pltpu.VMEM((16, N, 256), BF),
            pltpu.VMEM((4, 4, N, 256), BF),
            pltpu.VMEM((4, N, 256), BF),
            pltpu.VMEM((4, N, 256), BF),
            dma((12,)),
            dma((4, 2)),
            dma,
            dma,
            dma((16,)),
            dma,
            dma((SP,)),
            dma((SP,)),
            dma((16,)),
            dma((4, 4)),
            dma((4,)),
            dma((4,)),
        ],
        compiler_params=pltpu.CompilerParams(
            collective_id=0, has_side_effects=True, vmem_limit_bytes=60 * 1024 * 1024
        ),
    )(
        x_in, x_new, w_x, w_b, w_c, w_dt.T, w_z, conv_w,
        conv_b.reshape(1, -1), dt_bias.reshape(1, -1), a_log.reshape(1, -1),
        d_skip.reshape(1, -1), norm_g,
    )


def solution(mesh):
    return jax.shard_map(
        per_device,
        mesh=mesh,
        in_specs=(
            P("tp", "sp", None),
            P("sp", None),
            P(),
            P(),
            P(),
            P(),
            P(None, "tp"),
            P(),
            P(),
            P(),
            P(),
            P(),
            P("tp", None),
        ),
        out_specs=(P("sp", "tp", None, None), P("sp", "tp", None)),
        check_vma=False,
    )
```

```python
import jax
import jax.numpy as jnp
from jax import lax
from jax.experimental import pallas as pl
from jax.experimental.pallas import tpu as pltpu
from jax.sharding import PartitionSpec as P

H = 32
P_SIZE = 64
G = 8
N = 128
KW = 4
R = 4
D = 2048
T = 384
eps = 1e-05
MESH = pl.DeviceIdType.MESH
BF = jnp.bfloat16
F32 = jnp.float32
OFFS = (0, 1, 3, 2)
SP = 16


def dot(a, b):
    return jnp.dot(a, b, preferred_element_type=F32)


def dot_t(a, b):
    return lax.dot_general(a, b, (((1,), (1,)), ((), ())), preferred_element_type=F32)


def dot_exact(a, b):
    return jnp.dot(a, b, preferred_element_type=F32, precision=lax.Precision.HIGHEST)


def softplus(v):
    return jnp.maximum(v, 0.0) + jnp.log1p(jnp.exp(-jnp.abs(v)))


def kernel(
    x_hbm, xnew_hbm, wx_hbm, wb_hbm, wc_hbm, wdt_hbm, wz_hbm,
    cw_hbm, cb_hbm, dtb_hbm, alog_hbm, dskip_hbm, ng_hbm,
    st_out, ro_out,
    x_ref, xnew_ref, wx_ref, wb_ref, wc_ref, wdt_ref, wz_ref,
    cw_ref, cb_ref, dtb_ref, alog_ref, dskip_ref, ng_ref,
    pre_refs, key_refs, sc_refs, wg_ref, fac_ref,
    edge_tx, halo_rx, tail_rx, tot_tx, tot_rx,
    tx1, rx1, tx2, rx2,
    in_sems, w_sems,
    halo_s, halo_r, tail_s, tail_r, tot_s, tot_r, s1_s, s1_r, s2_s, s2_r,
):
    scope = jax.named_scope
    i = lax.axis_index("sp")
    j = lax.axis_index("tp")
    zp, xp = i // 4, i % 4
    yp, cp = j // 2, j % 2
    other = 1 - cp

    def pair(t):
        return (2 * yp + 4 - zp + OFFS[t]) % 4

    def load(src, dst, n):
        return pltpu.make_async_copy(src, dst, in_sems.at[n])

    first_loads = [
        load(x_hbm.at[0], x_ref.at[pl.ds(0, T), :], 0),
        load(x_hbm.at[1], x_ref.at[pl.ds(T, T), :], 1),
        load(wdt_hbm, wdt_ref, 2),
        load(dtb_hbm, dtb_ref, 3),
        load(alog_hbm, alog_ref, 4),
    ]
    conv_loads = [load(cw_hbm, cw_ref, 5), load(cb_hbm, cb_ref, 6)]
    last_loads = [
        load(xnew_hbm, xnew_ref, 7),
        load(dskip_hbm, dskip_ref, 8),
        load(ng_hbm, ng_ref, 9),
        load(wz_hbm, wz_ref, 10),
        load(wc_hbm.at[:, pl.ds(pl.multiple_of(j * N, N), N)], wc_ref, 11),
    ]

    def w_copy(t):
        q = pair(t)
        kcols = pl.ds(pl.multiple_of(q * 256, 256), 256)
        vcols = pl.ds(pl.multiple_of(q * 512, 512), 512)
        return [
            pltpu.make_async_copy(wb_hbm.at[:, kcols], wb_ref.at[:, kcols], w_sems.at[t, 0]),
            pltpu.make_async_copy(wx_hbm.at[:, vcols], wx_ref.at[:, vcols], w_sems.at[t, 1]),
        ]

    for c in first_loads + w_copy(0):
        c.start()

    bar = pltpu.get_barrier_semaphore()

    def sig(sp, tp):
        pl.semaphore_signal(bar, inc=1, device_id=(sp, tp), device_id_type=MESH)

    for d in range(1, SP):
        sig((i + d) % SP, j)

    @pl.when(cp != xp // 2)
    def _():
        for d in range(4):
            sig(zp * 4 + d, 2 * yp + other)

    for d in range(4):
        @pl.when((d != zp) | (yp != zp))
        def _():
            sig(d * 4 + xp, 2 * zp + cp)

    tail_tp = i // 2

    @pl.when((i != SP - 1) | (j != tail_tp))
    def _():
        sig(SP - 1, tail_tp)

    for c in conv_loads:
        c.start()

    with scope("xwait"):
        for c in first_loads:
            c.wait()
    for t in range(1, 4):
        for c in w_copy(t):
            c.start()
    for c in last_loads:
        c.start()
    lo = x_ref[T - 16:T, :].astype(F32)[13:16]
    hi = x_ref[2 * T - 16:2 * T, :].astype(F32)[13:16]
    edge_tx[...] = jnp.concatenate([lo, hi, jnp.zeros((2, D), F32)], axis=0).astype(BF)

    s1_self = (cp == xp // 2)
    arrivals = 15 + 2 + 4 - jnp.where(zp == yp, 1, 0)
    arrivals = arrivals + jnp.where(i == SP - 1, 16 - jnp.where(j == 7, 1, 0), 0)
    with scope("barrier"):
        pl.semaphore_wait(bar, arrivals)

    halo_copy = pltpu.make_async_remote_copy(
        edge_tx, halo_rx, halo_s, halo_r, device_id=((i + 1) % SP, j), device_id_type=MESH
    )

    @pl.when(i < SP - 1)
    def _():
        halo_copy.start()

    raw = dot_t(x_ref[0:2 * T, :], wdt_ref[...])
    steps = softplus(raw + dtb_ref[...])
    tot_tx[...] = jnp.zeros_like(tot_tx)
    rates = -jnp.exp(alog_ref[...])

    def tot_copy(d):
        return pltpu.make_async_remote_copy(
            tot_tx, tot_rx.at[i], tot_s.at[d], tot_r.at[i],
            device_id=((i + d) % SP, j), device_id_type=MESH,
        )

    upper = (
        lax.broadcasted_iota(jnp.int32, (T, T), 1) > lax.broadcasted_iota(jnp.int32, (T, T), 0)
    ).astype(F32).astype(BF)

    def weights(s):
        own = steps[T * s:T * (s + 1)]
        high = own.astype(BF)
        low = (own - high.astype(F32)).astype(BF)
        rest = dot(upper, high) + dot(upper, low)
        weight = jnp.exp(rates * rest) * own
        for g in range(G):
            wg_ref[g, T * s:T * (s + 1), 0:R] = weight[:, R * g:R * (g + 1)]

    def w_slice(t, u):
        q = pair(t)
        if u == 0:
            return wb_ref[:, pl.ds(pl.multiple_of(q * 256, 256), 256)]
        return wx_ref[:, pl.ds(pl.multiple_of(q * 512 + 256 * (u - 1), 256), 256)]

    def put_halo(pre, rows):
        for c in range(2):
            pre[c, 5:8, :] = rows[0:3, 128 * c:128 * (c + 1)]
            pre[c, T + 13:T + 16, :] = rows[3:6, 128 * c:128 * (c + 1)]

    def pre_of(n):
        return pre_refs[n % 6]

    def proj(n, s):
        t, u = n // 3, n % 3
        pre = pre_of(n)
        rows = T + 16 * s
        res = dot(x_ref[T * s:T * s + rows, :], w_slice(t, u))
        for c in range(2):
            pre[c, (T + 8) * s + 8:(T + 8) * (s + 1), :] = res[0:T, 128 * c:128 * (c + 1)]
        if s == 1:
            put_halo(pre, res[T:T + 8])

    with scope("w0wait"):
        for c in w_copy(0) + conv_loads:
            c.wait()

    proj(0, 0)
    for s in range(2):
        tot_tx[s:s + 1, 0:H] = jnp.sum(steps[T * s:T * (s + 1)], axis=0, keepdims=True)
    for d in range(1, SP):
        tot_copy(d).start()
    proj(1, 0)
    weights(0)
    proj(2, 0)

    with scope("halowait"):
        @pl.when(i > 0)
        def _():
            halo_copy.wait_recv()
        for c in w_copy(1):
            c.wait()
    halo = jnp.where(i > 0, halo_rx[...].astype(F32), 0.0)
    x_ref[2 * T:2 * T + 16, :] = jnp.concatenate([halo, jnp.zeros((8, D), F32)], axis=0).astype(BF)
    proj(0, 1)
    weights(1)
    proj(1, 1)
    proj(2, 1)

    lane = lax.broadcasted_iota(jnp.int32, (128, 128), 1)

    def conv(pre, s, c, r, off):
        cols = pl.ds(pl.multiple_of(off + 128 * c, 128), 128)
        taps = cw_ref[:, cols] * 0.5
        acc = cb_ref[:, cols] * 0.5 + taps[3:4] * pre[c, pl.ds((T + 8) * s + 8 + r, 128), :]
        for k in range(3):
            acc = acc + taps[k:k + 1] * pre[c, pl.ds((T + 8) * s + 5 + k + r, 128), :]
        return acc + acc * jnp.tanh(acc)

    def post_keys(t, s):
        q = pair(t)
        for c in range(2):
            for r in range(0, T, 128):
                out = conv(pre_of(3 * t), s, c, r, H * P_SIZE + q * 256)
                key_refs[t % 2][T * s + r:T * s + r + 128, 128 * c:128 * (c + 1)] = out.astype(BF)

    def post_values(t, b, s):
        g = 2 * pair(t) + b
        for c in range(2):
            for r in range(0, T, 128):
                out = conv(pre_of(3 * t + 1 + b), s, c, r, g * 256)
                w = wg_ref[g, pl.ds(T * s + r, 128), 0:R]
                w = jnp.where(lane < P_SIZE, w[:, 2 * c:2 * c + 1], w[:, 2 * c + 1:2 * c + 2])
                sc_refs[b][T * s + r:T * s + r + 128, 128 * c:128 * (c + 1)] = (out * w).astype(BF)

    def post(n, s):
        if n % 3 == 0:
            post_keys(n // 3, s)
        else:
            post_values(n // 3, n % 3 - 1, s)

    def s1_copy(t, a, b):
        n = 4 * t + 2 * a + b
        return pltpu.make_async_remote_copy(
            tx1.at[n], rx1.at[t, xp], s1_s.at[n], s1_r.at[t, xp],
            device_id=(zp * 4 + 2 * cp + a, 2 * yp + b), device_id_type=MESH,
        )

    def s1_own(a, b):
        return (xp == 2 * cp + a) & (cp == b)

    def contract(t, a, b):
        g = 2 * pair(t) + b
        keys = key_refs[t % 2][T * a:T * (a + 1), 128 * b:128 * (b + 1)]
        term = lax.dot_general(
            keys, sc_refs[b][T * a:T * (a + 1), :], (((0,), (0,)), ((), ())),
            preferred_element_type=F32,
        )
        term = term * fac_ref[g, a:a + 1, :]
        tx1[4 * t + 2 * a + b] = term.astype(BF)

    def send1(t, a, b):
        @pl.when(jnp.logical_not(s1_own(a, b)))
        def _():
            s1_copy(t, a, b).start()

        @pl.when(s1_own(a, b))
        def _():
            rx1[t, xp] = tx1[4 * t + 2 * a + b]

    def s2_copy(t):
        return pltpu.make_async_remote_copy(
            tx2.at[t], rx2.at[zp], s2_s.at[t], s2_r.at[zp],
            device_id=(yp * 4 + xp, 2 * pair(t) + cp), device_id_type=MESH,
        )

    def stage2(t):
        with scope("s1wait"):
            for d in range(4):
                @pl.when(jnp.logical_not((d == xp) & s1_self))
                def _():
                    pltpu.make_async_remote_copy(
                        tx1.at[0], rx1.at[t, d], s1_s.at[0], s1_r.at[t, d],
                        device_id=(i, j), device_id_type=MESH,
                    ).wait_recv()
        acc = rx1[t, 0].astype(F32)
        for d in range(1, 4):
            acc = acc + rx1[t, d].astype(F32)
        tx2[t] = acc.astype(BF)
        if OFFS[t] == 0:
            @pl.when(yp != zp)
            def _():
                s2_copy(t).start()

            @pl.when(yp == zp)
            def _():
                rx2[zp] = tx2[t]
        else:
            s2_copy(t).start()

    def factors():
        with scope("totwait"):
            for d in range(1, SP):
                src = (i + SP - d) % SP
                pltpu.make_async_remote_copy(
                    tot_tx, tot_rx.at[src], tot_s.at[d], tot_r.at[src],
                    device_id=((i + d) % SP, j), device_id_type=MESH,
                ).wait_recv()
        later = jnp.zeros((2, 128), F32)
        for d in range(SP):
            later = later + jnp.where(i < d, tot_rx[d], 0.0)
        factor = jnp.exp(rates * later[:, 0:H])
        spread = (
            lax.broadcasted_iota(jnp.int32, (H, H * P_SIZE), 1) // P_SIZE
            == lax.broadcasted_iota(jnp.int32, (H, H * P_SIZE), 0)
        ).astype(F32)
        wide = dot_exact(jnp.concatenate([factor, jnp.zeros((6, H), F32)], axis=0), spread)
        for g in range(G):
            fac_ref[g] = wide[:, 256 * g:256 * (g + 1)]

    def tail_copy(n):
        return pltpu.make_async_remote_copy(
            edge_tx, tail_rx, tail_s.at[n], tail_r,
            device_id=(2 * j + n % 2, n // 2), device_id_type=MESH,
        )

    def tail_self(n):
        return (j == 7) & (2 * j + n % 2 == i) & (n // 2 == j)

    def send_tails():
        @pl.when(i == SP - 1)
        def _():
            for n in range(16):
                @pl.when(jnp.logical_not(tail_self(n)))
                def _():
                    tail_copy(n).start()

        @pl.when((i == SP - 1) & (j == 7))
        def _():
            tail_rx[...] = edge_tx[...]

    slots = (
        (3, (0,)), (4, (1,)), (5, (2,)), (6, (3,)), (7, (4,)), (8, (5, 6)),
        (9, (7,)), (10, (8, 9)), (11, (10,)), (None, (11,)),
    )
    for k, (p, posts) in enumerate(slots):
        if p is not None and p % 3 == 0 and p > 3:
            with scope("wwait"):
                for c in w_copy(p // 3):
                    c.wait()
        with scope("slot"):
            for s in range(2):
                if p is not None:
                    proj(p, s)
                for n in posts:
                    post(n, s)
        if k == 1:
            factors()
        for n in posts:
            if n % 3:
                t, b = n // 3, n % 3 - 1
                for a in range(2):
                    contract(t, a, b)
                for a in range(2):
                    send1(t, a, b)
        if k == 3:
            send_tails()
        if k == 6:
            stage2(0)
        if k == 8:
            stage2(1)

    with scope("tailwait"):
        for c in last_loads:
            c.wait()

        @pl.when(jnp.logical_not((i == SP - 1) & (j == 7)))
        def _():
            tail_copy(0).wait_recv()

    ext = jnp.concatenate(
        [tail_rx[...].astype(F32), jnp.broadcast_to(xnew_ref[...].astype(F32), (8, D))], axis=0
    ).astype(BF)
    a_own = i % 2

    def fresh(w, off, width):
        res = dot(ext, w)
        cols = pl.ds(pl.multiple_of(off, 128), width)
        taps = cw_ref[:, cols] * 0.5
        acc = cb_ref[:, cols] * 0.5 + taps[3:4] * res[8:9]
        for k in range(3):
            acc = acc + taps[k:k + 1] * jnp.where(a_own == 0, res[k:k + 1], res[3 + k:4 + k])
        return acc + acc * jnp.tanh(acc)

    values = fresh(wx_ref[:, pl.ds(pl.multiple_of(j * 256, 256), 256)], j * 256, 256)
    keys = fresh(wb_ref[:, pl.ds(pl.multiple_of(j * N, N), N)], H * P_SIZE + j * N, N)
    query = fresh(wc_ref[...], H * P_SIZE + G * N + j * N, N)
    gate = dot(ext, wz_ref[...])[8:9]
    new_raw = dot_t(ext, wdt_ref[...])[8:9]
    new_steps = softplus(new_raw + dtb_ref[...])
    row = lax.broadcasted_iota(jnp.int32, (8, H), 0)
    packed = jnp.where(
        row == 0, new_steps, jnp.where(row == 1, jnp.exp(rates * new_steps), dskip_ref[...])
    )
    own_spread = (
        lax.broadcasted_iota(jnp.int32, (H, 256), 1) // P_SIZE + R * j
        == lax.broadcasted_iota(jnp.int32, (H, 256), 0)
    ).astype(F32)
    per_lane = dot_exact(packed, own_spread)
    step_row, decay_row, skip_row = per_lane[0:1], per_lane[1:2], per_lane[2:3]
    inner = jnp.sum(query * keys, axis=1, keepdims=True)
    direct = (step_row * inner + skip_row) * values
    gate = gate * jax.nn.sigmoid(gate)

    stage2(2)
    stage2(3)

    with scope("s2wait"):
        for d in range(4):
            @pl.when(jnp.logical_not((d == zp) & (yp == zp)))
            def _():
                pltpu.make_async_remote_copy(
                    tx2.at[0], rx2.at[d], s2_s.at[0], s2_r.at[d],
                    device_id=(i, j), device_id_type=MESH,
                ).wait_recv()
    state = rx2[0].astype(F32)
    for d in range(1, 4):
        state = state + rx2[d].astype(F32)
    st_out[0] = state.T.astype(BF).reshape(R, P_SIZE, N)
    held = dot_exact(jnp.broadcast_to(query, (8, N)), state)[0:1]
    gated = (decay_row * held + direct) * gate
    ms = jnp.sum(gated * gated, axis=1, keepdims=True) * (1.0 / 256)
    normed = gated * lax.rsqrt(ms + eps)
    head = lax.broadcasted_iota(jnp.int32, (R, 256), 0)
    chan = lax.broadcasted_iota(jnp.int32, (R, 256), 1) // P_SIZE
    split = jnp.where(head == chan, normed, 0.0)
    split = split[:, 0:128] + split[:, 128:256]
    split = split[:, 0:P_SIZE] + split[:, P_SIZE:128]
    ro_out[0] = (split * ng_ref[...]).astype(BF)

    with scope("drain"):
        @pl.when(i < SP - 1)
        def _():
            halo_copy.wait_send()

        for d in range(1, SP):
            tot_copy(d).wait_send()

        @pl.when(i == SP - 1)
        def _():
            for n in range(16):
                @pl.when(jnp.logical_not(tail_self(n)))
                def _():
                    tail_copy(n).wait_send()

        for t in range(4):
            for a in range(2):
                for b in range(2):
                    @pl.when(jnp.logical_not(s1_own(a, b)))
                    def _():
                        s1_copy(t, a, b).wait_send()
            if OFFS[t] == 0:
                @pl.when(yp != zp)
                def _():
                    s2_copy(t).wait_send()
            else:
                s2_copy(t).wait_send()


def per_device(
    x_in, x_new, w_x, w_b, w_c, w_dt, w_z, conv_w, conv_b, dt_bias, a_log, d_skip, norm_g
):
    hbm = pl.BlockSpec(memory_space=pl.ANY)
    vmem = pl.BlockSpec(memory_space=pltpu.VMEM)
    dma = pltpu.SemaphoreType.DMA
    return pl.pallas_call(
        kernel,
        out_shape=(
            pltpu.VMEM((1, R, P_SIZE, N), BF),
            pltpu.VMEM((1, R, P_SIZE), BF),
        ),
        in_specs=[hbm] * 13,
        out_specs=(vmem, vmem),
        scratch_shapes=[
            pltpu.VMEM((2 * T + 16, D), BF),
            pltpu.VMEM((1, D), BF),
            pltpu.VMEM((D, H * P_SIZE), BF),
            pltpu.VMEM((D, G * N), BF),
            pltpu.VMEM((D, N), BF),
            pltpu.VMEM((H, D), BF),
            pltpu.VMEM((D, 256), BF),
            pltpu.VMEM((KW, 4096), F32),
            pltpu.VMEM((1, 4096), F32),
            pltpu.VMEM((1, H), F32),
            pltpu.VMEM((1, H), F32),
            pltpu.VMEM((1, H), F32),
            pltpu.VMEM((R, P_SIZE), F32),
            [pltpu.VMEM((2, 2 * (T + 8), 128), F32) for _ in range(6)],
            [pltpu.VMEM((2 * T, 256), BF) for _ in range(2)],
            [pltpu.VMEM((2 * T, 256), BF) for _ in range(2)],
            pltpu.VMEM((G, 2 * T, 128), F32),
            pltpu.VMEM((G, 8, 256), F32),
            pltpu.VMEM((8, D), BF),
            pltpu.VMEM((8, D), BF),
            pltpu.VMEM((8, D), BF),
            pltpu.VMEM((2, 128), F32),
            pltpu.VMEM((SP, 2, 128), F32),
            pltpu.VMEM((16, N, 256), BF),
            pltpu.VMEM((4, 4, N, 256), BF),
            pltpu.VMEM((4, N, 256), BF),
            pltpu.VMEM((4, N, 256), BF),
            dma((12,)),
            dma((4, 2)),
            dma,
            dma,
            dma((16,)),
            dma,
            dma((SP,)),
            dma((SP,)),
            dma((16,)),
            dma((4, 4)),
            dma((4,)),
            dma((4,)),
        ],
        compiler_params=pltpu.CompilerParams(
            collective_id=0, has_side_effects=True, vmem_limit_bytes=60 * 1024 * 1024
        ),
    )(
        x_in, x_new, w_x, w_b, w_c, w_dt.T, w_z, conv_w,
        conv_b.reshape(1, -1), dt_bias.reshape(1, -1), a_log.reshape(1, -1),
        d_skip.reshape(1, -1), norm_g,
    )


def solution(mesh):
    return jax.shard_map(
        per_device,
        mesh=mesh,
        in_specs=(
            P("tp", "sp", None),
            P("sp", None),
            P(),
            P(),
            P(),
            P(),
            P(None, "tp"),
            P(),
            P(),
            P(),
            P(),
            P(),
            P("tp", None),
        ),
        out_specs=(P("sp", "tp", None, None), P("sp", "tp", None)),
        check_vma=False,
    )
```

```python
import jax
import jax.numpy as jnp
from jax import lax
from jax.experimental import pallas as pl
from jax.experimental.pallas import tpu as pltpu
from jax.sharding import PartitionSpec as P

H = 32
P_SIZE = 64
G = 8
N = 128
KW = 4
R = 4
D = 2048
T = 384
eps = 1e-05
MESH = pl.DeviceIdType.MESH
BF = jnp.bfloat16
F32 = jnp.float32
OFFS = (0, 1, 3, 2)
SP = 16


def dot(a, b):
    return jnp.dot(a, b, preferred_element_type=F32)


def dot_t(a, b):
    return lax.dot_general(a, b, (((1,), (1,)), ((), ())), preferred_element_type=F32)


def dot_exact(a, b):
    return jnp.dot(a, b, preferred_element_type=F32, precision=lax.Precision.HIGHEST)


def softplus(v):
    return jnp.maximum(v, 0.0) + jnp.log1p(jnp.exp(-jnp.abs(v)))


def kernel(
    x_hbm, xnew_hbm, wx_hbm, wb_hbm, wc_hbm, wdt_hbm, wz_hbm,
    cw_hbm, cb_hbm, dtb_hbm, alog_hbm, dskip_hbm, ng_hbm,
    st_out, ro_out,
    x_ref, xnew_ref, wx_ref, wb_ref, wc_ref, wdt_ref, wz_ref,
    cw_ref, cb_ref, dtb_ref, alog_ref, dskip_ref, ng_ref,
    pre_refs, key_refs, sc_refs, wg_ref, fac_ref,
    edge_tx, tail_tx, halo_rx, tail_rx, tot_tx, tot_rx,
    tx1, rx1, tx2, rx2,
    in_sems, w_sems,
    halo_s, halo_r, tail_s, tail_r, tot_s, tot_r, s1_s, s1_r, s2_s, s2_r,
):
    scope = jax.named_scope
    i = lax.axis_index("sp")
    j = lax.axis_index("tp")
    zp, xp = i // 4, i % 4
    yp, cp = j // 2, j % 2
    other = 1 - cp

    def pair(t):
        return (2 * yp + 4 - zp + OFFS[t]) % 4

    def load(src, dst, n):
        return pltpu.make_async_copy(src, dst, in_sems.at[n])

    first_loads = [
        load(x_hbm.at[0], x_ref.at[pl.ds(16, T), :], 0),
        load(wdt_hbm, wdt_ref, 2),
        load(dtb_hbm, dtb_ref, 3),
        load(alog_hbm, alog_ref, 4),
        load(x_hbm.at[1], x_ref.at[pl.ds(16 + T, T), :], 1),
    ]
    conv_loads = [load(cw_hbm, cw_ref, 5), load(cb_hbm, cb_ref, 6)]
    last_loads = [
        load(xnew_hbm, xnew_ref, 7),
        load(dskip_hbm, dskip_ref, 8),
        load(ng_hbm, ng_ref, 9),
        load(wz_hbm, wz_ref, 10),
        load(wc_hbm.at[:, pl.ds(pl.multiple_of(j * N, N), N)], wc_ref, 11),
    ]

    def w_copy(t):
        q = pair(t)
        kcols = pl.ds(pl.multiple_of(q * 256, 256), 256)
        vcols = pl.ds(pl.multiple_of(q * 512, 512), 512)
        return [
            pltpu.make_async_copy(wb_hbm.at[:, kcols], wb_ref.at[:, kcols], w_sems.at[t, 0]),
            pltpu.make_async_copy(wx_hbm.at[:, vcols], wx_ref.at[:, vcols], w_sems.at[t, 1]),
        ]

    for c in first_loads + w_copy(0):
        c.start()

    bar = pltpu.get_barrier_semaphore()

    def sig(sp, tp):
        pl.semaphore_signal(bar, inc=1, device_id=(sp, tp), device_id_type=MESH)

    for d in range(1, SP):
        sig((i + d) % SP, j)

    @pl.when(cp != xp // 2)
    def _():
        for d in range(4):
            sig(zp * 4 + d, 2 * yp + other)

    for d in range(4):
        @pl.when((d != zp) | (yp != zp))
        def _():
            sig(d * 4 + xp, 2 * zp + cp)

    tail_tp = i // 2

    @pl.when((i != SP - 1) | (j != tail_tp))
    def _():
        sig(SP - 1, tail_tp)

    for c in conv_loads:
        c.start()

    with scope("xwait"):
        for c in first_loads[:-1]:
            c.wait()
    raw0 = dot_t(x_ref[16:16 + T, :], wdt_ref[...])
    with scope("xwait"):
        first_loads[-1].wait()
    for t in range(1, 4):
        for c in w_copy(t):
            c.start()
    for c in last_loads:
        c.start()
    lo = x_ref[T:T + 16, :].astype(F32)[13:16]
    hi = x_ref[2 * T:2 * T + 16, :].astype(F32)[13:16]
    edge_tx[...] = jnp.concatenate([lo, hi, jnp.zeros((2, D), F32)], axis=0).astype(BF)

    s1_self = (cp == xp // 2)
    arrivals = 15 + 2 + 4 - jnp.where(zp == yp, 1, 0)
    arrivals = arrivals + jnp.where(i == SP - 1, 16 - jnp.where(j == 7, 1, 0), 0)
    with scope("barrier"):
        pl.semaphore_wait(bar, arrivals)

    halo_copy = pltpu.make_async_remote_copy(
        edge_tx, halo_rx, halo_s, halo_r, device_id=((i + 1) % SP, j), device_id_type=MESH
    )

    @pl.when(i < SP - 1)
    def _():
        halo_copy.start()

    def tail_copy(n):
        return pltpu.make_async_remote_copy(
            tail_tx.at[n % 2], tail_rx, tail_s.at[n], tail_r,
            device_id=(2 * j + n % 2, n // 2), device_id_type=MESH,
        )

    def tail_self(n):
        return (j == 7) & (2 * j + n % 2 == i) & (n // 2 == j)

    @pl.when(i == SP - 1)
    def _():
        tail_tx[0] = jnp.concatenate([lo, lo[0:1]], axis=0).astype(BF)
        tail_tx[1] = jnp.concatenate([hi, hi[0:1]], axis=0).astype(BF)
        for n in range(16):
            @pl.when(jnp.logical_not(tail_self(n)))
            def _():
                tail_copy(n).start()

    @pl.when((i == SP - 1) & (j == 7))
    def _():
        tail_rx[...] = tail_tx[1]

    raw = jnp.concatenate([raw0, dot_t(x_ref[16 + T:16 + 2 * T, :], wdt_ref[...])], axis=0)
    steps = softplus(raw + dtb_ref[...])
    tot_tx[...] = jnp.zeros_like(tot_tx)
    rates = -jnp.exp(alog_ref[...])

    def tot_copy(d):
        return pltpu.make_async_remote_copy(
            tot_tx, tot_rx.at[i], tot_s.at[d], tot_r.at[i],
            device_id=((i + d) % SP, j), device_id_type=MESH,
        )

    upper = (
        lax.broadcasted_iota(jnp.int32, (T, T), 1) > lax.broadcasted_iota(jnp.int32, (T, T), 0)
    ).astype(F32).astype(BF)

    def weights(s):
        own = steps[T * s:T * (s + 1)]
        high = own.astype(BF)
        low = (own - high.astype(F32)).astype(BF)
        rest = dot(upper, high) + dot(upper, low)
        weight = jnp.exp(rates * rest) * own
        for g in range(G):
            wg_ref[g, T * s:T * (s + 1), 0:R] = weight[:, R * g:R * (g + 1)]

    def w_slice(t, u):
        q = pair(t)
        if u == 0:
            return wb_ref[:, pl.ds(pl.multiple_of(q * 256, 256), 256)]
        return wx_ref[:, pl.ds(pl.multiple_of(q * 512 + 256 * (u - 1), 256), 256)]

    def put_halo(pre, rows):
        for c in range(2):
            pre[c, 5:8, :] = rows[0:3, 128 * c:128 * (c + 1)]
            pre[c, T + 13:T + 16, :] = rows[3:6, 128 * c:128 * (c + 1)]

    def pre_of(n):
        return pre_refs[n % 6]

    def proj(n, s):
        pre = pre_of(n)
        lead = 16 * (1 - s)
        start = (16 + T) * s
        res = dot(x_ref[start:start + T + lead, :], w_slice(n // 3, n % 3))
        for c in range(2):
            pre[c, (T + 8) * s + 8:(T + 8) * (s + 1), :] = res[lead:lead + T, 128 * c:128 * (c + 1)]
        if s == 0:
            put_halo(pre, res[0:8])

    with scope("w0wait"):
        for c in w_copy(0) + conv_loads:
            c.wait()

    proj(0, 1)
    for s in range(2):
        tot_tx[s:s + 1, 0:H] = jnp.sum(steps[T * s:T * (s + 1)], axis=0, keepdims=True)
    for d in range(1, SP):
        tot_copy(d).start()
    proj(1, 1)
    weights(0)
    proj(2, 1)

    with scope("halowait"):
        @pl.when(i > 0)
        def _():
            halo_copy.wait_recv()
        for c in w_copy(1):
            c.wait()
    halo = jnp.where(i > 0, halo_rx[...].astype(F32), 0.0)
    x_ref[0:16, :] = jnp.concatenate([halo, jnp.zeros((8, D), F32)], axis=0).astype(BF)
    proj(0, 0)
    weights(1)
    proj(1, 0)
    proj(2, 0)

    lane = lax.broadcasted_iota(jnp.int32, (128, 128), 1)

    def conv(pre, s, c, r, off):
        cols = pl.ds(pl.multiple_of(off + 128 * c, 128), 128)
        taps = cw_ref[:, cols] * 0.5
        acc = cb_ref[:, cols] * 0.5 + taps[3:4] * pre[c, pl.ds((T + 8) * s + 8 + r, 128), :]
        for k in range(3):
            acc = acc + taps[k:k + 1] * pre[c, pl.ds((T + 8) * s + 5 + k + r, 128), :]
        return acc + acc * jnp.tanh(acc)

    def post_keys(t, s):
        q = pair(t)
        for c in range(2):
            for r in range(0, T, 128):
                out = conv(pre_of(3 * t), s, c, r, H * P_SIZE + q * 256)
                key_refs[t % 2][T * s + r:T * s + r + 128, 128 * c:128 * (c + 1)] = out.astype(BF)

    def post_values(t, b, s):
        g = 2 * pair(t) + b
        for c in range(2):
            for r in range(0, T, 128):
                out = conv(pre_of(3 * t + 1 + b), s, c, r, g * 256)
                w = wg_ref[g, pl.ds(T * s + r, 128), 0:R]
                w = jnp.where(lane < P_SIZE, w[:, 2 * c:2 * c + 1], w[:, 2 * c + 1:2 * c + 2])
                sc_refs[b][T * s + r:T * s + r + 128, 128 * c:128 * (c + 1)] = (out * w).astype(BF)

    def post(n, s):
        if n % 3 == 0:
            post_keys(n // 3, s)
        else:
            post_values(n // 3, n % 3 - 1, s)

    def s1_copy(t, a, b):
        n = 4 * t + 2 * a + b
        return pltpu.make_async_remote_copy(
            tx1.at[n], rx1.at[t, xp], s1_s.at[n], s1_r.at[t, xp],
            device_id=(zp * 4 + 2 * cp + a, 2 * yp + b), device_id_type=MESH,
        )

    def s1_own(a, b):
        return (xp == 2 * cp + a) & (cp == b)

    def contract(t, a, b):
        g = 2 * pair(t) + b
        keys = key_refs[t % 2][T * a:T * (a + 1), 128 * b:128 * (b + 1)]
        term = lax.dot_general(
            keys, sc_refs[b][T * a:T * (a + 1), :], (((0,), (0,)), ((), ())),
            preferred_element_type=F32,
        )
        term = term * fac_ref[g, a:a + 1, :]
        tx1[4 * t + 2 * a + b] = term.astype(BF)

    def send1(t, a, b):
        @pl.when(jnp.logical_not(s1_own(a, b)))
        def _():
            s1_copy(t, a, b).start()

        @pl.when(s1_own(a, b))
        def _():
            rx1[t, xp] = tx1[4 * t + 2 * a + b]

    def s2_copy(t):
        return pltpu.make_async_remote_copy(
            tx2.at[t], rx2.at[zp], s2_s.at[t], s2_r.at[zp],
            device_id=(yp * 4 + xp, 2 * pair(t) + cp), device_id_type=MESH,
        )

    def stage2(t):
        with scope("s1wait"):
            for d in range(4):
                @pl.when(jnp.logical_not((d == xp) & s1_self))
                def _():
                    pltpu.make_async_remote_copy(
                        tx1.at[0], rx1.at[t, d], s1_s.at[0], s1_r.at[t, d],
                        device_id=(i, j), device_id_type=MESH,
                    ).wait_recv()
        acc = rx1[t, 0].astype(F32)
        for d in range(1, 4):
            acc = acc + rx1[t, d].astype(F32)
        tx2[t] = acc.astype(BF)
        if OFFS[t] == 0:
            @pl.when(yp != zp)
            def _():
                s2_copy(t).start()

            @pl.when(yp == zp)
            def _():
                rx2[zp] = tx2[t]
        else:
            s2_copy(t).start()

    def factors():
        with scope("totwait"):
            for d in range(1, SP):
                src = (i + SP - d) % SP
                pltpu.make_async_remote_copy(
                    tot_tx, tot_rx.at[src], tot_s.at[d], tot_r.at[src],
                    device_id=((i + d) % SP, j), device_id_type=MESH,
                ).wait_recv()
        later = jnp.zeros((2, 128), F32)
        for d in range(SP):
            later = later + jnp.where(i < d, tot_rx[d], 0.0)
        factor = jnp.exp(rates * later[:, 0:H])
        spread = (
            lax.broadcasted_iota(jnp.int32, (H, H * P_SIZE), 1) // P_SIZE
            == lax.broadcasted_iota(jnp.int32, (H, H * P_SIZE), 0)
        ).astype(F32)
        wide = dot_exact(jnp.concatenate([factor, jnp.zeros((6, H), F32)], axis=0), spread)
        for g in range(G):
            fac_ref[g] = wide[:, 256 * g:256 * (g + 1)]

    slots = (
        ("3a3b", "0a0b"), ("4a4b", "1a1b"), ("5a5b", "2a2b3a"), ("6a6b", "3b4a4b"),
        ("7a7b", "5a5b6a"), ("8a8b", "6b7a7b"), ("9a9b", "8a8b9a"), ("10a10b", "9b10a"),
        ("11a", "10b"), ("11b", "11a11b"),
    )

    def halves(text):
        out, num = [], ""
        for ch in text:
            if ch in "ab":
                out.append((int(num), "ab".index(ch)))
                num = ""
            else:
                num += ch
        return out

    for k, (projs, posts) in enumerate(slots):
        projs, posts = halves(projs), halves(posts)
        n = projs[0][0]
        if projs[0][1] == 0 and n % 3 == 0 and n > 3:
            with scope("wwait"):
                for c in w_copy(n // 3):
                    c.wait()
        if k == 1:
            factors()
        with scope("slot"):
            for m in range(max(len(projs), len(posts))):
                if m < len(projs):
                    proj(*projs[m])
                if m < len(posts):
                    n, half = posts[m]
                    post(n, half)
                    if n % 3:
                        contract(n // 3, half, n % 3 - 1)
        for n, half in posts:
            if n % 3 and half == 1:
                for a in range(2):
                    send1(n // 3, a, n % 3 - 1)
        if k == 6:
            stage2(0)
        if k == 8:
            stage2(1)

    with scope("tailwait"):
        for c in last_loads:
            c.wait()

        @pl.when(jnp.logical_not((i == SP - 1) & (j == 7)))
        def _():
            tail_copy(0).wait_recv()

    ext = jnp.concatenate(
        [tail_rx[...].astype(F32), jnp.broadcast_to(xnew_ref[...].astype(F32), (12, D))], axis=0
    ).astype(BF)

    def fresh(w, off, width):
        res = dot(ext, w)
        cols = pl.ds(pl.multiple_of(off, 128), width)
        taps = cw_ref[:, cols] * 0.5
        acc = cb_ref[:, cols] * 0.5 + taps[3:4] * res[8:9]
        for k in range(3):
            acc = acc + taps[k:k + 1] * res[k:k + 1]
        return acc + acc * jnp.tanh(acc)

    values = fresh(wx_ref[:, pl.ds(pl.multiple_of(j * 256, 256), 256)], j * 256, 256)
    keys = fresh(wb_ref[:, pl.ds(pl.multiple_of(j * N, N), N)], H * P_SIZE + j * N, N)
    query = fresh(wc_ref[...], H * P_SIZE + G * N + j * N, N)
    gate = dot(ext, wz_ref[...])[8:9]
    new_raw = dot_t(ext, wdt_ref[...])[8:9]
    new_steps = softplus(new_raw + dtb_ref[...])
    row = lax.broadcasted_iota(jnp.int32, (8, H), 0)
    packed = jnp.where(
        row == 0, new_steps, jnp.where(row == 1, jnp.exp(rates * new_steps), dskip_ref[...])
    )
    own_spread = (
        lax.broadcasted_iota(jnp.int32, (H, 256), 1) // P_SIZE + R * j
        == lax.broadcasted_iota(jnp.int32, (H, 256), 0)
    ).astype(F32)
    per_lane = dot_exact(packed, own_spread)
    step_row, decay_row, skip_row = per_lane[0:1], per_lane[1:2], per_lane[2:3]
    inner = jnp.sum(query * keys, axis=1, keepdims=True)
    direct = (step_row * inner + skip_row) * values
    gate = gate * jax.nn.sigmoid(gate)

    stage2(2)
    stage2(3)

    with scope("s2wait"):
        for d in range(4):
            @pl.when(jnp.logical_not((d == zp) & (yp == zp)))
            def _():
                pltpu.make_async_remote_copy(
                    tx2.at[0], rx2.at[d], s2_s.at[0], s2_r.at[d],
                    device_id=(i, j), device_id_type=MESH,
                ).wait_recv()
    state = rx2[0].astype(F32)
    for d in range(1, 4):
        state = state + rx2[d].astype(F32)
    st_out[0] = state.T.astype(BF).reshape(R, P_SIZE, N)
    held = dot_exact(jnp.broadcast_to(query, (8, N)), state)[0:1]
    gated = (decay_row * held + direct) * gate
    ms = jnp.sum(gated * gated, axis=1, keepdims=True) * (1.0 / 256)
    normed = gated * lax.rsqrt(ms + eps)
    head = lax.broadcasted_iota(jnp.int32, (R, 256), 0)
    chan = lax.broadcasted_iota(jnp.int32, (R, 256), 1) // P_SIZE
    split = jnp.where(head == chan, normed, 0.0)
    split = split[:, 0:128] + split[:, 128:256]
    split = split[:, 0:P_SIZE] + split[:, P_SIZE:128]
    ro_out[0] = (split * ng_ref[...]).astype(BF)

    with scope("drain"):
        @pl.when(i < SP - 1)
        def _():
            halo_copy.wait_send()

        for d in range(1, SP):
            tot_copy(d).wait_send()

        @pl.when(i == SP - 1)
        def _():
            for n in range(16):
                @pl.when(jnp.logical_not(tail_self(n)))
                def _():
                    tail_copy(n).wait_send()

        for t in range(4):
            for a in range(2):
                for b in range(2):
                    @pl.when(jnp.logical_not(s1_own(a, b)))
                    def _():
                        s1_copy(t, a, b).wait_send()
            if OFFS[t] == 0:
                @pl.when(yp != zp)
                def _():
                    s2_copy(t).wait_send()
            else:
                s2_copy(t).wait_send()


def per_device(
    x_in, x_new, w_x, w_b, w_c, w_dt, w_z, conv_w, conv_b, dt_bias, a_log, d_skip, norm_g
):
    hbm = pl.BlockSpec(memory_space=pl.ANY)
    vmem = pl.BlockSpec(memory_space=pltpu.VMEM)
    dma = pltpu.SemaphoreType.DMA
    return pl.pallas_call(
        kernel,
        out_shape=(
            pltpu.VMEM((1, R, P_SIZE, N), BF),
            pltpu.VMEM((1, R, P_SIZE), BF),
        ),
        in_specs=[hbm] * 13,
        out_specs=(vmem, vmem),
        scratch_shapes=[
            pltpu.VMEM((2 * T + 16, D), BF),
            pltpu.VMEM((1, D), BF),
            pltpu.VMEM((D, H * P_SIZE), BF),
            pltpu.VMEM((D, G * N), BF),
            pltpu.VMEM((D, N), BF),
            pltpu.VMEM((H, D), BF),
            pltpu.VMEM((D, 256), BF),
            pltpu.VMEM((KW, 4096), F32),
            pltpu.VMEM((1, 4096), F32),
            pltpu.VMEM((1, H), F32),
            pltpu.VMEM((1, H), F32),
            pltpu.VMEM((1, H), F32),
            pltpu.VMEM((R, P_SIZE), F32),
            [pltpu.VMEM((2, 2 * (T + 8), 128), F32) for _ in range(6)],
            [pltpu.VMEM((2 * T, 256), BF) for _ in range(2)],
            [pltpu.VMEM((2 * T, 256), BF) for _ in range(2)],
            pltpu.VMEM((G, 2 * T, 128), F32),
            pltpu.VMEM((G, 8, 256), F32),
            pltpu.VMEM((8, D), BF),
            pltpu.VMEM((2, 4, D), BF),
            pltpu.VMEM((8, D), BF),
            pltpu.VMEM((4, D), BF),
            pltpu.VMEM((2, 128), F32),
            pltpu.VMEM((SP, 2, 128), F32),
            pltpu.VMEM((16, N, 256), BF),
            pltpu.VMEM((4, 4, N, 256), BF),
            pltpu.VMEM((4, N, 256), BF),
            pltpu.VMEM((4, N, 256), BF),
            dma((12,)),
            dma((4, 2)),
            dma,
            dma,
            dma((16,)),
            dma,
            dma((SP,)),
            dma((SP,)),
            dma((16,)),
            dma((4, 4)),
            dma((4,)),
            dma((4,)),
        ],
        compiler_params=pltpu.CompilerParams(
            collective_id=0, has_side_effects=True, vmem_limit_bytes=60 * 1024 * 1024
        ),
    )(
        x_in, x_new, w_x, w_b, w_c, w_dt.T, w_z, conv_w,
        conv_b.reshape(1, -1), dt_bias.reshape(1, -1), a_log.reshape(1, -1),
        d_skip.reshape(1, -1), norm_g,
    )


def solution(mesh):
    return jax.shard_map(
        per_device,
        mesh=mesh,
        in_specs=(
            P("tp", "sp", None),
            P("sp", None),
            P(),
            P(),
            P(),
            P(),
            P(None, "tp"),
            P(),
            P(),
            P(),
            P(),
            P(),
            P("tp", None),
        ),
        out_specs=(P("sp", "tp", None, None), P("sp", "tp", None)),
        check_vma=False,
    )
```

```python
import jax
import jax.numpy as jnp
from jax import lax
from jax.experimental import pallas as pl
from jax.experimental.pallas import tpu as pltpu
from jax.sharding import PartitionSpec as P

H = 32
P_SIZE = 64
G = 8
N = 128
KW = 4
R = 4
D = 2048
T = 384
eps = 1e-05
MESH = pl.DeviceIdType.MESH
BF = jnp.bfloat16
F32 = jnp.float32
OFFS = (0, 1, 3, 2)
SP = 16


def dot(a, b):
    return jnp.dot(a, b, preferred_element_type=F32)


def dot_t(a, b):
    return lax.dot_general(a, b, (((1,), (1,)), ((), ())), preferred_element_type=F32)


def dot_exact(a, b):
    return jnp.dot(a, b, preferred_element_type=F32, precision=lax.Precision.HIGHEST)


def softplus(v):
    return jnp.maximum(v, 0.0) + jnp.log1p(jnp.exp(-jnp.abs(v)))


def kernel(
    x_hbm, xnew_hbm, wx_hbm, wb_hbm, wc_hbm, wdt_hbm, wz_hbm,
    cw_hbm, cb_hbm, dtb_hbm, alog_hbm, dskip_hbm, ng_hbm,
    st_out, ro_out,
    x_ref, xnew_ref, w_ref, wc_ref, wdt_ref, wz_ref,
    cw_ref, cb_ref, dtb_ref, alog_ref, dskip_ref, ng_ref,
    pre_refs, key_refs, sc_refs, wg_ref, fac_ref,
    edge_tx, tail_tx, halo_rx, tail_rx, tot_tx, tot_rx,
    tx1, rx1, tx2, rx2,
    in_sems, w_sems,
    halo_s, halo_r, tail_s, tail_r, tot_s, tot_r, s1_s, s1_r, s2_s, s2_r,
):
    scope = jax.named_scope
    i = lax.axis_index("sp")
    j = lax.axis_index("tp")
    zp, xp = i // 4, i % 4
    yp, cp = j // 2, j % 2
    other = 1 - cp

    def pair(t):
        return (2 * yp + 4 - zp + OFFS[t]) % 4

    def load(src, dst, n):
        return pltpu.make_async_copy(src, dst, in_sems.at[n])

    first_loads = [
        load(x_hbm.at[0], x_ref.at[pl.ds(16, T), :], 0),
        load(wdt_hbm, wdt_ref, 2),
        load(dtb_hbm, dtb_ref, 3),
        load(alog_hbm, alog_ref, 4),
        load(x_hbm.at[1], x_ref.at[pl.ds(16 + T, T), :], 1),
    ]
    conv_loads = [load(cw_hbm, cw_ref, 5), load(cb_hbm, cb_ref, 6)]
    last_loads = [
        load(xnew_hbm, xnew_ref, 7),
        load(dskip_hbm, dskip_ref, 8),
        load(ng_hbm, ng_ref, 9),
        load(wz_hbm, wz_ref, 10),
        load(wc_hbm.at[:, pl.ds(pl.multiple_of(j * N, N), N)], wc_ref, 11),
    ]

    def w_copy(t):
        q = pair(t)
        kcols = pl.ds(pl.multiple_of(q * 256, 256), 256)
        vcols = pl.ds(pl.multiple_of(q * 512, 512), 512)
        return [
            pltpu.make_async_copy(
                wb_hbm.at[:, kcols], w_ref.at[:, pl.ds(768 * t, 256)], w_sems.at[t, 0]
            ),
            pltpu.make_async_copy(
                wx_hbm.at[:, vcols], w_ref.at[:, pl.ds(768 * t + 256, 512)], w_sems.at[t, 1]
            ),
        ]

    for c in first_loads + w_copy(0):
        c.start()

    bar = pltpu.get_barrier_semaphore()

    def sig(sp, tp):
        pl.semaphore_signal(bar, inc=1, device_id=(sp, tp), device_id_type=MESH)

    for d in range(1, SP):
        sig((i + d) % SP, j)

    @pl.when(cp != xp // 2)
    def _():
        for d in range(4):
            sig(zp * 4 + d, 2 * yp + other)

    for d in range(4):
        @pl.when((d != zp) | (yp != zp))
        def _():
            sig(d * 4 + xp, 2 * zp + cp)

    tail_tp = i // 2

    @pl.when((i != SP - 1) | (j != tail_tp))
    def _():
        sig(SP - 1, tail_tp)

    for c in conv_loads:
        c.start()

    with scope("xwait"):
        for c in first_loads[:-1]:
            c.wait()
    raw0 = dot_t(x_ref[16:16 + T, :], wdt_ref[...])
    with scope("xwait"):
        first_loads[-1].wait()
    for t in range(1, 4):
        for c in w_copy(t):
            c.start()
    for c in last_loads:
        c.start()
    lo = x_ref[T:T + 16, :].astype(F32)[13:16]
    hi = x_ref[2 * T:2 * T + 16, :].astype(F32)[13:16]
    edge_tx[...] = jnp.concatenate([lo, hi, jnp.zeros((2, D), F32)], axis=0).astype(BF)

    s1_self = (cp == xp // 2)
    arrivals = 15 + 2 + 4 - jnp.where(zp == yp, 1, 0)
    arrivals = arrivals + jnp.where(i == SP - 1, 16 - jnp.where(j == 7, 1, 0), 0)
    with scope("barrier"):
        pl.semaphore_wait(bar, arrivals)

    halo_copy = pltpu.make_async_remote_copy(
        edge_tx, halo_rx, halo_s, halo_r, device_id=((i + 1) % SP, j), device_id_type=MESH
    )

    @pl.when(i < SP - 1)
    def _():
        halo_copy.start()

    def tail_copy(n):
        return pltpu.make_async_remote_copy(
            tail_tx.at[n % 2], tail_rx, tail_s.at[n], tail_r,
            device_id=(2 * j + n % 2, n // 2), device_id_type=MESH,
        )

    def tail_self(n):
        return (j == 7) & (2 * j + n % 2 == i) & (n // 2 == j)

    @pl.when(i == SP - 1)
    def _():
        tail_tx[0] = jnp.concatenate([lo, lo[0:1]], axis=0).astype(BF)
        tail_tx[1] = jnp.concatenate([hi, hi[0:1]], axis=0).astype(BF)
        for n in range(16):
            @pl.when(jnp.logical_not(tail_self(n)))
            def _():
                tail_copy(n).start()

    @pl.when((i == SP - 1) & (j == 7))
    def _():
        tail_rx[...] = tail_tx[1]

    raw = jnp.concatenate([raw0, dot_t(x_ref[16 + T:16 + 2 * T, :], wdt_ref[...])], axis=0)
    steps = softplus(raw + dtb_ref[...])
    tot_tx[...] = jnp.zeros_like(tot_tx)
    rates = -jnp.exp(alog_ref[...])

    def tot_copy(d):
        return pltpu.make_async_remote_copy(
            tot_tx, tot_rx.at[i], tot_s.at[d], tot_r.at[i],
            device_id=((i + d) % SP, j), device_id_type=MESH,
        )

    upper = (
        lax.broadcasted_iota(jnp.int32, (T, T), 1) > lax.broadcasted_iota(jnp.int32, (T, T), 0)
    ).astype(F32).astype(BF)

    def rests():
        parts = []
        for s in range(2):
            own = steps[T * s:T * (s + 1)]
            high = own.astype(BF).astype(F32)
            parts += [high, own - high]
        res = dot(upper, jnp.concatenate(parts, axis=1).astype(BF))
        return [res[:, 64 * s:64 * s + H] + res[:, 64 * s + H:64 * s + 2 * H] for s in range(2)]

    def weights(s, rest):
        weight = jnp.exp(rates * rest) * steps[T * s:T * (s + 1)]
        for g in range(G):
            wg_ref[g, T * s:T * (s + 1), 0:R] = weight[:, R * g:R * (g + 1)]

    def put_halo(pre, rows):
        for c in range(2):
            pre[c, 5:8, :] = rows[0:3, 128 * c:128 * (c + 1)]
            pre[c, T + 13:T + 16, :] = rows[3:6, 128 * c:128 * (c + 1)]

    def pre_of(n):
        return pre_refs[n % 6]

    def proj(n, count, s):
        lead = 16 * (1 - s)
        start = (16 + T) * s
        wide = dot(x_ref[start:start + T + lead, :], w_ref[:, 256 * n:256 * (n + count)])
        for k in range(count):
            pre = pre_of(n + k)
            res = wide[:, 256 * k:256 * (k + 1)]
            for c in range(2):
                pre[c, (T + 8) * s + 8:(T + 8) * (s + 1), :] = (
                    res[lead:lead + T, 128 * c:128 * (c + 1)]
                )
            if s == 0:
                put_halo(pre, res[0:8])

    for s in range(2):
        tot_tx[s:s + 1, 0:H] = jnp.sum(steps[T * s:T * (s + 1)], axis=0, keepdims=True)
    for d in range(1, SP):
        tot_copy(d).start()
    with scope("w0wait"):
        for c in w_copy(0) + conv_loads:
            c.wait()

    proj(0, 2, 1)
    proj(2, 1, 1)
    rest_sums = rests()
    weights(0, rest_sums[0])
    weights(1, rest_sums[1])

    with scope("halowait"):
        @pl.when(i > 0)
        def _():
            halo_copy.wait_recv()
        for c in w_copy(1):
            c.wait()
    halo = jnp.where(i > 0, halo_rx[...].astype(F32), 0.0)
    x_ref[0:16, :] = jnp.concatenate([halo, jnp.zeros((8, D), F32)], axis=0).astype(BF)
    proj(0, 2, 0)
    proj(2, 1, 0)

    lane = lax.broadcasted_iota(jnp.int32, (128, 128), 1)

    def conv(pre, s, c, r, off):
        cols = pl.ds(pl.multiple_of(off + 128 * c, 128), 128)
        taps = cw_ref[:, cols] * 0.5
        acc = cb_ref[:, cols] * 0.5 + taps[3:4] * pre[c, pl.ds((T + 8) * s + 8 + r, 128), :]
        for k in range(3):
            acc = acc + taps[k:k + 1] * pre[c, pl.ds((T + 8) * s + 5 + k + r, 128), :]
        return acc + acc * jnp.tanh(acc)

    def post_keys(t, s):
        q = pair(t)
        for c in range(2):
            for r in range(0, T, 128):
                out = conv(pre_of(3 * t), s, c, r, H * P_SIZE + q * 256)
                key_refs[t % 2][T * s + r:T * s + r + 128, 128 * c:128 * (c + 1)] = out.astype(BF)

    def post_values(t, b, s):
        g = 2 * pair(t) + b
        for c in range(2):
            for r in range(0, T, 128):
                out = conv(pre_of(3 * t + 1 + b), s, c, r, g * 256)
                w = wg_ref[g, pl.ds(T * s + r, 128), 0:R]
                w = jnp.where(lane < P_SIZE, w[:, 2 * c:2 * c + 1], w[:, 2 * c + 1:2 * c + 2])
                sc_refs[b][T * s + r:T * s + r + 128, 128 * c:128 * (c + 1)] = (out * w).astype(BF)

    def post(n, s):
        if n % 3 == 0:
            post_keys(n // 3, s)
        else:
            post_values(n // 3, n % 3 - 1, s)

    def s1_copy(t, a, b):
        n = 4 * t + 2 * a + b
        return pltpu.make_async_remote_copy(
            tx1.at[n], rx1.at[t, xp], s1_s.at[n], s1_r.at[t, xp],
            device_id=(zp * 4 + 2 * cp + a, 2 * yp + b), device_id_type=MESH,
        )

    def s1_own(a, b):
        return (xp == 2 * cp + a) & (cp == b)

    def contract(t, a, b):
        g = 2 * pair(t) + b
        keys = key_refs[t % 2][T * a:T * (a + 1), 128 * b:128 * (b + 1)]
        term = lax.dot_general(
            keys, sc_refs[b][T * a:T * (a + 1), :], (((0,), (0,)), ((), ())),
            preferred_element_type=F32,
        )
        term = term * fac_ref[g, a:a + 1, :]
        tx1[4 * t + 2 * a + b] = term.astype(BF)

    def s1_half(a, b, h):
        n = 12 + 2 * a + b
        cols = pl.ds(128 * h, 128)
        return pltpu.make_async_remote_copy(
            tx1.at[n, :, cols], rx1.at[3, xp, :, cols], s1_s.at[n + 4 * h], s1_r.at[3 + h, xp],
            device_id=(zp * 4 + 2 * cp + a, 2 * yp + b), device_id_type=MESH,
        )

    def s1_sends(t, a, b):
        return [s1_half(a, b, h) for h in range(2)] if t == 3 else [s1_copy(t, a, b)]

    def send1(t, a, b):
        @pl.when(jnp.logical_not(s1_own(a, b)))
        def _():
            for c in s1_sends(t, a, b):
                c.start()

        @pl.when(s1_own(a, b))
        def _():
            rx1[t, xp] = tx1[4 * t + 2 * a + b]

    def s2_copy(t):
        return pltpu.make_async_remote_copy(
            tx2.at[t], rx2.at[zp], s2_s.at[t], s2_r.at[zp],
            device_id=(yp * 4 + xp, 2 * pair(t) + cp), device_id_type=MESH,
        )

    def stage2(t):
        with scope("s1wait"):
            for d in range(4):
                @pl.when(jnp.logical_not((d == xp) & s1_self))
                def _():
                    pltpu.make_async_remote_copy(
                        tx1.at[0], rx1.at[t, d], s1_s.at[0], s1_r.at[t, d],
                        device_id=(i, j), device_id_type=MESH,
                    ).wait_recv()
        acc = rx1[t, 0].astype(F32)
        for d in range(1, 4):
            acc = acc + rx1[t, d].astype(F32)
        tx2[t] = acc.astype(BF)
        if OFFS[t] == 0:
            @pl.when(yp != zp)
            def _():
                s2_copy(t).start()

            @pl.when(yp == zp)
            def _():
                rx2[zp] = tx2[t]
        else:
            s2_copy(t).start()

    def s2_half(h):
        cols = pl.ds(128 * h, 128)
        return pltpu.make_async_remote_copy(
            tx2.at[3, :, cols], rx2.at[zp, :, cols], s2_s.at[3 + h], s2_r.at[zp],
            device_id=(yp * 4 + xp, 2 * pair(3) + cp), device_id_type=MESH,
        )

    def stage2_last():
        for h in range(2):
            cols = pl.ds(128 * h, 128)
            with scope("s1wait"):
                for d in range(4):
                    @pl.when(jnp.logical_not((d == xp) & s1_self))
                    def _():
                        pltpu.make_async_remote_copy(
                            tx1.at[0, :, cols], rx1.at[3, d, :, cols],
                            s1_s.at[0], s1_r.at[3 + h, d],
                            device_id=(i, j), device_id_type=MESH,
                        ).wait_recv()
            acc = rx1[3, 0, :, cols].astype(F32)
            for d in range(1, 4):
                acc = acc + rx1[3, d, :, cols].astype(F32)
            tx2[3, :, cols] = acc.astype(BF)
            s2_half(h).start()

    def factors():
        with scope("totwait"):
            for d in range(1, SP):
                src = (i + SP - d) % SP
                pltpu.make_async_remote_copy(
                    tot_tx, tot_rx.at[src], tot_s.at[d], tot_r.at[src],
                    device_id=((i + d) % SP, j), device_id_type=MESH,
                ).wait_recv()
        later = jnp.zeros((2, 128), F32)
        for d in range(SP):
            later = later + jnp.where(i < d, tot_rx[d], 0.0)
        factor = jnp.exp(rates * later[:, 0:H])
        first = lax.broadcasted_iota(jnp.int32, (2, 128), 1) < P_SIZE
        for g in range(G):
            for c in range(2):
                h = R * g + 2 * c
                fac_ref[g, 0:2, 128 * c:128 * (c + 1)] = jnp.where(
                    first, factor[:, h:h + 1], factor[:, h + 1:h + 2]
                )

    slots = (
        ((3, 2, 0), "0a0b"), ((3, 2, 1), "1a1b"), ((5, 2, 0), "2a2b3a"), ((5, 2, 1), "3b4a4b"),
        ((7, 2, 0), "5a5b6a"), ((7, 2, 1), "6b7a"), ((9, 2, 0), "7b8a8b"), ((9, 2, 1), "9a9b"),
        ((11, 1, 0), "10a10b"), ((11, 1, 1), "11a"), (None, "11b"),
    )

    def halves(text):
        out, num = [], ""
        for ch in text:
            if ch in "ab":
                out.append((int(num), "ab".index(ch)))
                num = ""
            else:
                num += ch
        return out

    for k, (project_unit, posts) in enumerate(slots):
        posts = halves(posts)
        if k in (2, 6):
            with scope("wwait"):
                for c in w_copy(2 if k == 2 else 3):
                    c.wait()
        if k == 1:
            factors()
        with scope("slot"):
            if project_unit is not None:
                proj(*project_unit)
            for n, half in posts:
                post(n, half)
                if n % 3:
                    contract(n // 3, half, n % 3 - 1)
        for n, half in posts:
            if n % 3:
                send1(n // 3, half, n % 3 - 1)
        if k == 6:
            stage2(0)
        if k == 8:
            stage2(1)

    with scope("tailwait"):
        for c in last_loads:
            c.wait()

        @pl.when(jnp.logical_not((i == SP - 1) & (j == 7)))
        def _():
            tail_copy(0).wait_recv()

    ext = jnp.concatenate(
        [tail_rx[...].astype(F32), jnp.broadcast_to(xnew_ref[...].astype(F32), (12, D))], axis=0
    ).astype(BF)

    def fresh(w, off, width):
        res = dot(ext, w)
        cols = pl.ds(pl.multiple_of(off, 128), width)
        taps = cw_ref[:, cols] * 0.5
        acc = cb_ref[:, cols] * 0.5 + taps[3:4] * res[8:9]
        for k in range(3):
            acc = acc + taps[k:k + 1] * res[k:k + 1]
        return acc + acc * jnp.tanh(acc)

    turn = (zp + 4 - yp) % 4
    place = 768 * (turn + (turn // 2) * (1 - 2 * (turn % 2)))
    vcols = pl.ds(pl.multiple_of(place + 256 + 256 * cp, 256), 256)
    kcols = pl.ds(pl.multiple_of(place + N * cp, N), N)
    values = fresh(w_ref[:, vcols], j * 256, 256)
    keys = fresh(w_ref[:, kcols], H * P_SIZE + j * N, N)
    query = fresh(wc_ref[...], H * P_SIZE + G * N + j * N, N)
    gate = dot(ext, wz_ref[...])[8:9]
    new_raw = dot_t(ext, wdt_ref[...])[8:9]
    new_steps = softplus(new_raw + dtb_ref[...])
    row = lax.broadcasted_iota(jnp.int32, (8, H), 0)
    packed = jnp.where(
        row == 0, new_steps, jnp.where(row == 1, jnp.exp(rates * new_steps), dskip_ref[...])
    )
    own_spread = (
        lax.broadcasted_iota(jnp.int32, (H, 256), 1) // P_SIZE + R * j
        == lax.broadcasted_iota(jnp.int32, (H, 256), 0)
    ).astype(F32)
    per_lane = dot_exact(packed, own_spread)
    step_row, decay_row, skip_row = per_lane[0:1], per_lane[1:2], per_lane[2:3]
    inner = jnp.sum(query * keys, axis=1, keepdims=True)
    direct = (step_row * inner + skip_row) * values
    gate = gate * jax.nn.sigmoid(gate)

    stage2(2)
    stage2_last()

    with scope("s2wait"):
        for d in range(4):
            @pl.when(jnp.logical_not((d == zp) & (yp == zp)))
            def _():
                pltpu.make_async_remote_copy(
                    tx2.at[0], rx2.at[d], s2_s.at[0], s2_r.at[d],
                    device_id=(i, j), device_id_type=MESH,
                ).wait_recv()
    state = rx2[0].astype(F32)
    for d in range(1, 4):
        state = state + rx2[d].astype(F32)
    st_out[0] = state.T.astype(BF).reshape(R, P_SIZE, N)
    held = dot_exact(jnp.broadcast_to(query, (8, N)), state)[0:1]
    gated = (decay_row * held + direct) * gate
    ms = jnp.sum(gated * gated, axis=1, keepdims=True) * (1.0 / 256)
    normed = gated * lax.rsqrt(ms + eps)
    head = lax.broadcasted_iota(jnp.int32, (R, 256), 0)
    chan = lax.broadcasted_iota(jnp.int32, (R, 256), 1) // P_SIZE
    split = jnp.where(head == chan, normed, 0.0)
    split = split[:, 0:128] + split[:, 128:256]
    split = split[:, 0:P_SIZE] + split[:, P_SIZE:128]
    ro_out[0] = (split * ng_ref[...]).astype(BF)

    with scope("drain"):
        @pl.when(i < SP - 1)
        def _():
            halo_copy.wait_send()

        for d in range(1, SP):
            tot_copy(d).wait_send()

        @pl.when(i == SP - 1)
        def _():
            for n in range(16):
                @pl.when(jnp.logical_not(tail_self(n)))
                def _():
                    tail_copy(n).wait_send()

        for t in range(4):
            for a in range(2):
                for b in range(2):
                    @pl.when(jnp.logical_not(s1_own(a, b)))
                    def _():
                        for c in s1_sends(t, a, b):
                            c.wait_send()
            if OFFS[t] == 0:
                @pl.when(yp != zp)
                def _():
                    s2_copy(t).wait_send()
            elif t == 3:
                for h in range(2):
                    s2_half(h).wait_send()
            else:
                s2_copy(t).wait_send()


def per_device(
    x_in, x_new, w_x, w_b, w_c, w_dt, w_z, conv_w, conv_b, dt_bias, a_log, d_skip, norm_g
):
    hbm = pl.BlockSpec(memory_space=pl.ANY)
    vmem = pl.BlockSpec(memory_space=pltpu.VMEM)
    dma = pltpu.SemaphoreType.DMA
    return pl.pallas_call(
        kernel,
        out_shape=(
            pltpu.VMEM((1, R, P_SIZE, N), BF),
            pltpu.VMEM((1, R, P_SIZE), BF),
        ),
        in_specs=[hbm] * 13,
        out_specs=(vmem, vmem),
        scratch_shapes=[
            pltpu.VMEM((2 * T + 16, D), BF),
            pltpu.VMEM((1, D), BF),
            pltpu.VMEM((D, H * P_SIZE + G * N), BF),
            pltpu.VMEM((D, N), BF),
            pltpu.VMEM((H, D), BF),
            pltpu.VMEM((D, 256), BF),
            pltpu.VMEM((KW, 4096), F32),
            pltpu.VMEM((1, 4096), F32),
            pltpu.VMEM((1, H), F32),
            pltpu.VMEM((1, H), F32),
            pltpu.VMEM((1, H), F32),
            pltpu.VMEM((R, P_SIZE), F32),
            [pltpu.VMEM((2, 2 * (T + 8), 128), F32) for _ in range(6)],
            [pltpu.VMEM((2 * T, 256), BF) for _ in range(2)],
            [pltpu.VMEM((2 * T, 256), BF) for _ in range(2)],
            pltpu.VMEM((G, 2 * T, 128), F32),
            pltpu.VMEM((G, 8, 256), F32),
            pltpu.VMEM((8, D), BF),
            pltpu.VMEM((2, 4, D), BF),
            pltpu.VMEM((8, D), BF),
            pltpu.VMEM((4, D), BF),
            pltpu.VMEM((2, 128), F32),
            pltpu.VMEM((SP, 2, 128), F32),
            pltpu.VMEM((16, N, 256), BF),
            pltpu.VMEM((4, 4, N, 256), BF),
            pltpu.VMEM((4, N, 256), BF),
            pltpu.VMEM((4, N, 256), BF),
            dma((12,)),
            dma((4, 2)),
            dma,
            dma,
            dma((16,)),
            dma,
            dma((SP,)),
            dma((SP,)),
            dma((20,)),
            dma((5, 4)),
            dma((5,)),
            dma((4,)),
        ],
        compiler_params=pltpu.CompilerParams(
            collective_id=0, has_side_effects=True, vmem_limit_bytes=60 * 1024 * 1024
        ),
    )(
        x_in, x_new, w_x, w_b, w_c, w_dt.T, w_z, conv_w,
        conv_b.reshape(1, -1), dt_bias.reshape(1, -1), a_log.reshape(1, -1),
        d_skip.reshape(1, -1), norm_g,
    )


def solution(mesh):
    return jax.shard_map(
        per_device,
        mesh=mesh,
        in_specs=(
            P("tp", "sp", None),
            P("sp", None),
            P(),
            P(),
            P(),
            P(),
            P(None, "tp"),
            P(),
            P(),
            P(),
            P(),
            P(),
            P("tp", None),
        ),
        out_specs=(P("sp", "tp", None, None), P("sp", "tp", None)),
        check_vma=False,
    )
```

```python
import jax
import jax.numpy as jnp
from jax import lax
from jax.experimental import pallas as pl
from jax.experimental.pallas import tpu as pltpu
from jax.sharding import PartitionSpec as P

H = 32
P_SIZE = 64
G = 8
N = 128
KW = 4
R = 4
D = 2048
T = 384
eps = 1e-05
MESH = pl.DeviceIdType.MESH
BF = jnp.bfloat16
F32 = jnp.float32
OFFS = (0, 1, 3, 2)
SP = 16


def dot(a, b):
    return jnp.dot(a, b, preferred_element_type=F32)


def dot_t(a, b):
    return lax.dot_general(a, b, (((1,), (1,)), ((), ())), preferred_element_type=F32)


def dot_exact(a, b):
    return jnp.dot(a, b, preferred_element_type=F32, precision=lax.Precision.HIGHEST)


def softplus(v):
    return jnp.maximum(v, 0.0) + jnp.log1p(jnp.exp(-jnp.abs(v)))


def kernel(
    x_hbm, xnew_hbm, wx_hbm, wb_hbm, wc_hbm, wdt_hbm, wz_hbm,
    cw_hbm, cb_hbm, dtb_hbm, alog_hbm, dskip_hbm, ng_hbm,
    st_out, ro_out,
    x_ref, xnew_ref, w_ref, wc_ref, wdt_ref, wz_ref,
    cw_ref, cb_ref, dtb_ref, alog_ref, dskip_ref, ng_ref,
    pre_refs, key_refs, sc_refs, wg_ref, fac_ref,
    edge_tx, tail_tx, halo_rx, tail_rx, tot_tx, tot_rx,
    tx1, rx1, tx2, rx2,
    in_sems, w_sems,
    halo_s, halo_r, tail_s, tail_r, tot_s, tot_r, s1_s, s1_r, s2_s, s2_r,
):
    scope = jax.named_scope
    i = lax.axis_index("sp")
    j = lax.axis_index("tp")
    zp, xp = i // 4, i % 4
    yp, cp = j // 2, j % 2
    other = 1 - cp

    def pair(t):
        return (2 * yp + 4 - zp + OFFS[t]) % 4

    def load(src, dst, n):
        return pltpu.make_async_copy(src, dst, in_sems.at[n])

    first_loads = [
        load(x_hbm.at[0], x_ref.at[pl.ds(16, T), :], 0),
        load(wdt_hbm, wdt_ref, 2),
        load(dtb_hbm, dtb_ref, 3),
        load(alog_hbm, alog_ref, 4),
        load(x_hbm.at[1], x_ref.at[pl.ds(16 + T, T), :], 1),
    ]
    conv_loads = [load(cw_hbm, cw_ref, 5), load(cb_hbm, cb_ref, 6)]
    last_loads = [
        load(xnew_hbm, xnew_ref, 7),
        load(dskip_hbm, dskip_ref, 8),
        load(ng_hbm, ng_ref, 9),
        load(wz_hbm, wz_ref, 10),
        load(wc_hbm.at[:, pl.ds(pl.multiple_of(j * N, N), N)], wc_ref, 11),
    ]

    def w_copy(t):
        q = pair(t)
        kcols = pl.ds(pl.multiple_of(q * 256, 256), 256)
        vcols = pl.ds(pl.multiple_of(q * 512, 512), 512)
        return [
            pltpu.make_async_copy(
                wb_hbm.at[:, kcols], w_ref.at[:, pl.ds(768 * t, 256)], w_sems.at[t, 0]
            ),
            pltpu.make_async_copy(
                wx_hbm.at[:, vcols], w_ref.at[:, pl.ds(768 * t + 256, 512)], w_sems.at[t, 1]
            ),
        ]

    for c in first_loads + w_copy(0):
        c.start()

    bar = pltpu.get_barrier_semaphore()

    def sig(sp, tp):
        pl.semaphore_signal(bar, inc=1, device_id=(sp, tp), device_id_type=MESH)

    for d in range(1, SP):
        sig((i + d) % SP, j)

    @pl.when(cp != xp // 2)
    def _():
        for d in range(4):
            sig(zp * 4 + d, 2 * yp + other)

    for d in range(4):
        @pl.when((d != zp) | (yp != zp))
        def _():
            sig(d * 4 + xp, 2 * zp + cp)

    tail_tp = i // 2

    @pl.when((i != SP - 1) | (j != tail_tp))
    def _():
        sig(SP - 1, tail_tp)

    for c in conv_loads:
        c.start()

    with scope("xwait"):
        for c in first_loads[:-1]:
            c.wait()
    raw0 = dot_t(x_ref[16:16 + T, :], wdt_ref[...])
    with scope("xwait"):
        first_loads[-1].wait()
    for t in range(1, 4):
        for c in w_copy(t):
            c.start()
    for c in last_loads:
        c.start()
    lo = x_ref[T:T + 16, :].astype(F32)[13:16]
    hi = x_ref[2 * T:2 * T + 16, :].astype(F32)[13:16]
    edge_tx[...] = jnp.concatenate([lo, hi, jnp.zeros((2, D), F32)], axis=0).astype(BF)

    s1_self = (cp == xp // 2)
    arrivals = 15 + 2 + 4 - jnp.where(zp == yp, 1, 0)
    arrivals = arrivals + jnp.where(i == SP - 1, 16 - jnp.where(j == 7, 1, 0), 0)
    with scope("barrier"):
        pl.semaphore_wait(bar, arrivals)

    halo_copy = pltpu.make_async_remote_copy(
        edge_tx, halo_rx, halo_s, halo_r, device_id=((i + 1) % SP, j), device_id_type=MESH
    )

    @pl.when(i < SP - 1)
    def _():
        halo_copy.start()

    raw = jnp.concatenate([raw0, dot_t(x_ref[16 + T:16 + 2 * T, :], wdt_ref[...])], axis=0)
    steps = softplus(raw + dtb_ref[...])
    tot_tx[...] = jnp.zeros_like(tot_tx)
    rates = -jnp.exp(alog_ref[...])

    def tot_copy(d):
        return pltpu.make_async_remote_copy(
            tot_tx, tot_rx.at[i], tot_s.at[d], tot_r.at[i],
            device_id=((i + d) % SP, j), device_id_type=MESH,
        )

    upper = (
        lax.broadcasted_iota(jnp.int32, (T, T), 1) > lax.broadcasted_iota(jnp.int32, (T, T), 0)
    ).astype(F32).astype(BF)

    def rests():
        parts = []
        for s in range(2):
            own = steps[T * s:T * (s + 1)]
            high = own.astype(BF).astype(F32)
            parts += [high, own - high]
        res = dot(upper, jnp.concatenate(parts, axis=1).astype(BF))
        return [res[:, 64 * s:64 * s + H] + res[:, 64 * s + H:64 * s + 2 * H] for s in range(2)]

    def weights(s, rest):
        weight = jnp.exp(rates * rest) * steps[T * s:T * (s + 1)]
        for g in range(G):
            wg_ref[g, T * s:T * (s + 1), 0:R] = weight[:, R * g:R * (g + 1)]

    def put_halo(pre, rows):
        for c in range(2):
            pre[c, 5:8, :] = rows[0:3, 128 * c:128 * (c + 1)]
            pre[c, T + 13:T + 16, :] = rows[3:6, 128 * c:128 * (c + 1)]

    def pre_of(n):
        return pre_refs[n % 6]

    def proj(n, count, s):
        lead = 16 * (1 - s)
        start = (16 + T) * s
        wide = dot(x_ref[start:start + T + lead, :], w_ref[:, 256 * n:256 * (n + count)])
        for k in range(count):
            pre = pre_of(n + k)
            res = wide[:, 256 * k:256 * (k + 1)]
            for c in range(2):
                pre[c, (T + 8) * s + 8:(T + 8) * (s + 1), :] = (
                    res[lead:lead + T, 128 * c:128 * (c + 1)]
                )
            if s == 0:
                put_halo(pre, res[0:8])

    for s in range(2):
        tot_tx[s:s + 1, 0:H] = jnp.sum(steps[T * s:T * (s + 1)], axis=0, keepdims=True)
    for d in range(1, SP):
        tot_copy(d).start()
    def tail_copy(n):
        return pltpu.make_async_remote_copy(
            tail_tx.at[n % 2], tail_rx, tail_s.at[n], tail_r,
            device_id=(2 * j + n % 2, n // 2), device_id_type=MESH,
        )

    def tail_self(n):
        return (j == 7) & (2 * j + n % 2 == i) & (n // 2 == j)

    @pl.when(i == SP - 1)
    def _():
        tail_tx[0] = jnp.concatenate([lo, lo[0:1]], axis=0).astype(BF)
        tail_tx[1] = jnp.concatenate([hi, hi[0:1]], axis=0).astype(BF)
        for n in range(16):
            @pl.when(jnp.logical_not(tail_self(n)))
            def _():
                tail_copy(n).start()

    @pl.when((i == SP - 1) & (j == 7))
    def _():
        tail_rx[...] = tail_tx[1]

    with scope("w0wait"):
        for c in w_copy(0) + conv_loads:
            c.wait()

    proj(0, 2, 1)
    proj(2, 1, 1)
    rest_sums = rests()
    weights(0, rest_sums[0])
    weights(1, rest_sums[1])

    with scope("halowait"):
        @pl.when(i > 0)
        def _():
            halo_copy.wait_recv()
        for c in w_copy(1):
            c.wait()
    halo = jnp.where(i > 0, halo_rx[...].astype(F32), 0.0)
    x_ref[0:16, :] = jnp.concatenate([halo, jnp.zeros((8, D), F32)], axis=0).astype(BF)
    proj(0, 2, 0)
    proj(2, 1, 0)

    lane = lax.broadcasted_iota(jnp.int32, (128, 128), 1)

    def conv(pre, s, c, r, off):
        cols = pl.ds(pl.multiple_of(off + 128 * c, 128), 128)
        taps = cw_ref[:, cols] * 0.5
        acc = cb_ref[:, cols] * 0.5 + taps[3:4] * pre[c, pl.ds((T + 8) * s + 8 + r, 128), :]
        for k in range(3):
            acc = acc + taps[k:k + 1] * pre[c, pl.ds((T + 8) * s + 5 + k + r, 128), :]
        return acc + acc * jnp.tanh(acc)

    def post_keys(t, s):
        q = pair(t)
        for c in range(2):
            for r in range(0, T, 128):
                out = conv(pre_of(3 * t), s, c, r, H * P_SIZE + q * 256)
                key_refs[t % 2][T * s + r:T * s + r + 128, 128 * c:128 * (c + 1)] = out.astype(BF)

    def post_values(t, b, s):
        g = 2 * pair(t) + b
        for c in range(2):
            for r in range(0, T, 128):
                out = conv(pre_of(3 * t + 1 + b), s, c, r, g * 256)
                w = wg_ref[g, pl.ds(T * s + r, 128), 0:R]
                w = jnp.where(lane < P_SIZE, w[:, 2 * c:2 * c + 1], w[:, 2 * c + 1:2 * c + 2])
                sc_refs[b][T * s + r:T * s + r + 128, 128 * c:128 * (c + 1)] = (out * w).astype(BF)

    def post(n, s):
        if n % 3 == 0:
            post_keys(n // 3, s)
        else:
            post_values(n // 3, n % 3 - 1, s)

    def s1_copy(t, a, b):
        n = 4 * t + 2 * a + b
        return pltpu.make_async_remote_copy(
            tx1.at[n], rx1.at[t, xp], s1_s.at[n], s1_r.at[t, xp],
            device_id=(zp * 4 + 2 * cp + a, 2 * yp + b), device_id_type=MESH,
        )

    def s1_own(a, b):
        return (xp == 2 * cp + a) & (cp == b)

    def contract(t, a, b):
        g = 2 * pair(t) + b
        keys = key_refs[t % 2][T * a:T * (a + 1), 128 * b:128 * (b + 1)]
        term = lax.dot_general(
            keys, sc_refs[b][T * a:T * (a + 1), :], (((0,), (0,)), ((), ())),
            preferred_element_type=F32,
        )
        term = term * fac_ref[g, a:a + 1, :]
        tx1[4 * t + 2 * a + b] = term.astype(BF)

    def s1_half(a, b, h):
        n = 12 + 2 * a + b
        cols = pl.ds(128 * h, 128)
        return pltpu.make_async_remote_copy(
            tx1.at[n, :, cols], rx1.at[3, xp, :, cols], s1_s.at[n + 4 * h], s1_r.at[3 + h, xp],
            device_id=(zp * 4 + 2 * cp + a, 2 * yp + b), device_id_type=MESH,
        )

    def s1_sends(t, a, b):
        return [s1_half(a, b, h) for h in range(2)] if t == 3 else [s1_copy(t, a, b)]

    def send1(t, a, b):
        @pl.when(jnp.logical_not(s1_own(a, b)))
        def _():
            for c in s1_sends(t, a, b):
                c.start()

        @pl.when(s1_own(a, b))
        def _():
            rx1[t, xp] = tx1[4 * t + 2 * a + b]

    def s2_copy(t):
        return pltpu.make_async_remote_copy(
            tx2.at[t], rx2.at[zp], s2_s.at[t], s2_r.at[zp],
            device_id=(yp * 4 + xp, 2 * pair(t) + cp), device_id_type=MESH,
        )

    def stage2(t):
        with scope("s1wait"):
            for d in range(4):
                @pl.when(jnp.logical_not((d == xp) & s1_self))
                def _():
                    pltpu.make_async_remote_copy(
                        tx1.at[0], rx1.at[t, d], s1_s.at[0], s1_r.at[t, d],
                        device_id=(i, j), device_id_type=MESH,
                    ).wait_recv()
        acc = rx1[t, 0].astype(F32)
        for d in range(1, 4):
            acc = acc + rx1[t, d].astype(F32)
        tx2[t] = acc.astype(BF)
        if OFFS[t] == 0:
            @pl.when(yp != zp)
            def _():
                s2_copy(t).start()

            @pl.when(yp == zp)
            def _():
                rx2[zp] = tx2[t]
        else:
            s2_copy(t).start()

    def s2_half(h):
        cols = pl.ds(128 * h, 128)
        return pltpu.make_async_remote_copy(
            tx2.at[3, :, cols], rx2.at[zp, :, cols], s2_s.at[3 + h], s2_r.at[zp],
            device_id=(yp * 4 + xp, 2 * pair(3) + cp), device_id_type=MESH,
        )

    def stage2_last():
        for h in range(2):
            cols = pl.ds(128 * h, 128)
            with scope("s1wait"):
                for d in range(4):
                    @pl.when(jnp.logical_not((d == xp) & s1_self))
                    def _():
                        pltpu.make_async_remote_copy(
                            tx1.at[0, :, cols], rx1.at[3, d, :, cols],
                            s1_s.at[0], s1_r.at[3 + h, d],
                            device_id=(i, j), device_id_type=MESH,
                        ).wait_recv()
            acc = rx1[3, 0, :, cols].astype(F32)
            for d in range(1, 4):
                acc = acc + rx1[3, d, :, cols].astype(F32)
            tx2[3, :, cols] = acc.astype(BF)
            s2_half(h).start()

    def factors():
        with scope("totwait"):
            for d in range(1, SP):
                src = (i + SP - d) % SP
                pltpu.make_async_remote_copy(
                    tot_tx, tot_rx.at[src], tot_s.at[d], tot_r.at[src],
                    device_id=((i + d) % SP, j), device_id_type=MESH,
                ).wait_recv()
        later = jnp.zeros((2, 128), F32)
        for d in range(SP):
            later = later + jnp.where(i < d, tot_rx[d], 0.0)
        factor = jnp.exp(rates * later[:, 0:H])
        first = lax.broadcasted_iota(jnp.int32, (2, 128), 1) < P_SIZE
        for g in range(G):
            for c in range(2):
                h = R * g + 2 * c
                fac_ref[g, 0:2, 128 * c:128 * (c + 1)] = jnp.where(
                    first, factor[:, h:h + 1], factor[:, h + 1:h + 2]
                )

    slots = (
        ((3, 2, 0), "0a0b"), ((3, 2, 1), "1a1b"), ((5, 2, 0), "2a2b3a"), ((5, 2, 1), "3b4a4b"),
        ((7, 2, 0), "5a5b6a"), ((7, 2, 1), "6b7a"), ((9, 2, 0), "7b8a8b"), ((9, 2, 1), "9a9b"),
        ((11, 1, 0), "10a10b"), ((11, 1, 1), "11a"), (None, "11b"),
    )

    def halves(text):
        out, num = [], ""
        for ch in text:
            if ch in "ab":
                out.append((int(num), "ab".index(ch)))
                num = ""
            else:
                num += ch
        return out

    for k, (project_unit, posts) in enumerate(slots):
        posts = halves(posts)
        if k in (2, 6):
            with scope("wwait"):
                for c in w_copy(2 if k == 2 else 3):
                    c.wait()
        if k == 1:
            factors()
        with scope("slot"):
            if project_unit is not None:
                proj(*project_unit)
            for n, half in posts:
                post(n, half)
                if n % 3:
                    contract(n // 3, half, n % 3 - 1)
        for n, half in posts:
            if n % 3:
                send1(n // 3, half, n % 3 - 1)
        if k == 6:
            stage2(0)
        if k == 8:
            stage2(1)

    with scope("tailwait"):
        for c in last_loads:
            c.wait()

        @pl.when(jnp.logical_not((i == SP - 1) & (j == 7)))
        def _():
            tail_copy(0).wait_recv()

    ext = jnp.concatenate(
        [tail_rx[...].astype(F32), jnp.broadcast_to(xnew_ref[...].astype(F32), (12, D))], axis=0
    ).astype(BF)

    def fresh(w, off, width):
        res = dot(ext, w)
        cols = pl.ds(pl.multiple_of(off, 128), width)
        taps = cw_ref[:, cols] * 0.5
        acc = cb_ref[:, cols] * 0.5 + taps[3:4] * res[8:9]
        for k in range(3):
            acc = acc + taps[k:k + 1] * res[k:k + 1]
        return acc + acc * jnp.tanh(acc)

    turn = (zp + 4 - yp) % 4
    place = 768 * (turn + (turn // 2) * (1 - 2 * (turn % 2)))
    vcols = pl.ds(pl.multiple_of(place + 256 + 256 * cp, 256), 256)
    kcols = pl.ds(pl.multiple_of(place + N * cp, N), N)
    values = fresh(w_ref[:, vcols], j * 256, 256)
    keys = fresh(w_ref[:, kcols], H * P_SIZE + j * N, N)
    query = fresh(wc_ref[...], H * P_SIZE + G * N + j * N, N)
    gate = dot(ext, wz_ref[...])[8:9]
    new_raw = dot_t(ext, wdt_ref[...])[8:9]
    new_steps = softplus(new_raw + dtb_ref[...])
    row = lax.broadcasted_iota(jnp.int32, (8, H), 0)
    packed = jnp.where(
        row == 0, new_steps, jnp.where(row == 1, jnp.exp(rates * new_steps), dskip_ref[...])
    )
    own_spread = (
        lax.broadcasted_iota(jnp.int32, (H, 256), 1) // P_SIZE + R * j
        == lax.broadcasted_iota(jnp.int32, (H, 256), 0)
    ).astype(F32)
    per_lane = dot_exact(packed, own_spread)
    step_row, decay_row, skip_row = per_lane[0:1], per_lane[1:2], per_lane[2:3]
    inner = jnp.sum(query * keys, axis=1, keepdims=True)
    direct = (step_row * inner + skip_row) * values
    gate = gate * jax.nn.sigmoid(gate)

    stage2(2)
    stage2_last()

    with scope("s2wait"):
        for d in range(4):
            @pl.when(jnp.logical_not((d == zp) & (yp == zp)))
            def _():
                pltpu.make_async_remote_copy(
                    tx2.at[0], rx2.at[d], s2_s.at[0], s2_r.at[d],
                    device_id=(i, j), device_id_type=MESH,
                ).wait_recv()
    state = rx2[0].astype(F32)
    for d in range(1, 4):
        state = state + rx2[d].astype(F32)
    st_out[0] = state.T.astype(BF).reshape(R, P_SIZE, N)
    held = dot_exact(jnp.broadcast_to(query, (8, N)), state)[0:1]
    gated = (decay_row * held + direct) * gate
    ms = jnp.sum(gated * gated, axis=1, keepdims=True) * (1.0 / 256)
    normed = gated * lax.rsqrt(ms + eps)
    head = lax.broadcasted_iota(jnp.int32, (R, 256), 0)
    chan = lax.broadcasted_iota(jnp.int32, (R, 256), 1) // P_SIZE
    split = jnp.where(head == chan, normed, 0.0)
    split = split[:, 0:128] + split[:, 128:256]
    split = split[:, 0:P_SIZE] + split[:, P_SIZE:128]
    ro_out[0] = (split * ng_ref[...]).astype(BF)

    with scope("drain"):
        @pl.when(i < SP - 1)
        def _():
            halo_copy.wait_send()

        for d in range(1, SP):
            tot_copy(d).wait_send()

        @pl.when(i == SP - 1)
        def _():
            for n in range(16):
                @pl.when(jnp.logical_not(tail_self(n)))
                def _():
                    tail_copy(n).wait_send()

        for t in range(4):
            for a in range(2):
                for b in range(2):
                    @pl.when(jnp.logical_not(s1_own(a, b)))
                    def _():
                        for c in s1_sends(t, a, b):
                            c.wait_send()
            if OFFS[t] == 0:
                @pl.when(yp != zp)
                def _():
                    s2_copy(t).wait_send()
            elif t == 3:
                for h in range(2):
                    s2_half(h).wait_send()
            else:
                s2_copy(t).wait_send()


def per_device(
    x_in, x_new, w_x, w_b, w_c, w_dt, w_z, conv_w, conv_b, dt_bias, a_log, d_skip, norm_g
):
    hbm = pl.BlockSpec(memory_space=pl.ANY)
    vmem = pl.BlockSpec(memory_space=pltpu.VMEM)
    dma = pltpu.SemaphoreType.DMA
    return pl.pallas_call(
        kernel,
        out_shape=(
            pltpu.VMEM((1, R, P_SIZE, N), BF),
            pltpu.VMEM((1, R, P_SIZE), BF),
        ),
        in_specs=[hbm] * 13,
        out_specs=(vmem, vmem),
        scratch_shapes=[
            pltpu.VMEM((2 * T + 16, D), BF),
            pltpu.VMEM((1, D), BF),
            pltpu.VMEM((D, H * P_SIZE + G * N), BF),
            pltpu.VMEM((D, N), BF),
            pltpu.VMEM((H, D), BF),
            pltpu.VMEM((D, 256), BF),
            pltpu.VMEM((KW, 4096), F32),
            pltpu.VMEM((1, 4096), F32),
            pltpu.VMEM((1, H), F32),
            pltpu.VMEM((1, H), F32),
            pltpu.VMEM((1, H), F32),
            pltpu.VMEM((R, P_SIZE), F32),
            [pltpu.VMEM((2, 2 * (T + 8), 128), F32) for _ in range(6)],
            [pltpu.VMEM((2 * T, 256), BF) for _ in range(2)],
            [pltpu.VMEM((2 * T, 256), BF) for _ in range(2)],
            pltpu.VMEM((G, 2 * T, 128), F32),
            pltpu.VMEM((G, 8, 256), F32),
            pltpu.VMEM((8, D), BF),
            pltpu.VMEM((2, 4, D), BF),
            pltpu.VMEM((8, D), BF),
            pltpu.VMEM((4, D), BF),
            pltpu.VMEM((2, 128), F32),
            pltpu.VMEM((SP, 2, 128), F32),
            pltpu.VMEM((16, N, 256), BF),
            pltpu.VMEM((4, 4, N, 256), BF),
            pltpu.VMEM((4, N, 256), BF),
            pltpu.VMEM((4, N, 256), BF),
            dma((12,)),
            dma((4, 2)),
            dma,
            dma,
            dma((16,)),
            dma,
            dma((SP,)),
            dma((SP,)),
            dma((20,)),
            dma((5, 4)),
            dma((5,)),
            dma((4,)),
        ],
        compiler_params=pltpu.CompilerParams(
            collective_id=0, has_side_effects=True, vmem_limit_bytes=60 * 1024 * 1024
        ),
    )(
        x_in, x_new, w_x, w_b, w_c, w_dt.T, w_z, conv_w,
        conv_b.reshape(1, -1), dt_bias.reshape(1, -1), a_log.reshape(1, -1),
        d_skip.reshape(1, -1), norm_g,
    )


def solution(mesh):
    return jax.shard_map(
        per_device,
        mesh=mesh,
        in_specs=(
            P("tp", "sp", None),
            P("sp", None),
            P(),
            P(),
            P(),
            P(),
            P(None, "tp"),
            P(),
            P(),
            P(),
            P(),
            P(),
            P("tp", None),
        ),
        out_specs=(P("sp", "tp", None, None), P("sp", "tp", None)),
        check_vma=False,
    )
```
